32 devices in a mesh: ep: 16 (over z, y, x), tp: 2 (over core).
Axes of the slice: x: 2, y: 2, z: 4, core: 2. Of those that a mesh axis runs over, the one named last changes fastest.
Arguments:
- tokens: bfloat16 [256, 2048], P(('ep', 'tp')), may hold values from -6 to 6
- mix_gain: float32 [2048], replicated, may hold values from 0.1 to 1.9
- w_query: bfloat16 [2048, 16, 128], P(None, 'tp', 'ep'), may hold values from -0.125 to 0.125
- w_key: bfloat16 [2048, 16, 128], P(None, 'tp', 'ep'), may hold values from -0.125 to 0.125
- w_value: bfloat16 [2048, 16, 128], P(None, 'tp', 'ep'), may hold values from -0.125 to 0.125
- w_zgate: bfloat16 [2048, 16, 128], P(None, 'tp', 'ep'), may hold values from -0.125 to 0.125
- w_beta: bfloat16 [2048, 16], P(None, 'tp'), may hold values from -0.125 to 0.125
- w_decay: bfloat16 [2048, 16], P(None, 'tp'), may hold values from -0.125 to 0.125
- decay_rate: float32 [16], P('tp'), may hold values from 0.5 to 8
- decay_bias: float32 [16], P('tp'), may hold values from -3 to 0
- head_gain: float32 [128], replicated, may hold values from 0.1 to 1.9
- state: float32 [256, 16, 128, 128], P('ep', 'tp'), may hold values from -1.5 to 1.5
- w_out: bfloat16 [2048, 2048], P('tp', 'ep'), may hold values from -0.125 to 0.125
- moe_gain: float32 [2048], replicated, may hold values from 0.1 to 1.9
- dense_mix: bfloat16 [2048], replicated, may hold values from -0.125 to 0.125
- dense_gate: bfloat16 [2048, 4096], P(None, ('ep', 'tp')), may hold values from -0.125 to 0.125
- dense_up: bfloat16 [2048, 4096], P(None, ('ep', 'tp')), may hold values from -0.125 to 0.125
- dense_down: bfloat16 [4096, 2048], P(('ep', 'tp')), may hold values from -0.09375 to 0.09375
- expert_gate: bfloat16 [16, 2048, 1024], P('ep', None, 'tp'), may hold values from -0.125 to 0.125
- expert_up: bfloat16 [16, 2048, 1024], P('ep', None, 'tp'), may hold values from -0.125 to 0.125
- expert_down: bfloat16 [16, 1024, 2048], P('ep', 'tp'), may hold values from -0.1875 to 0.1875
- expert_ids: int32 [256, 4], replicated, may hold values from 0 to 15, as said below
- route_weight: float32 [256, 4], replicated, may hold values from 0.1 to 1
Outputs:
- layer_out: bfloat16 [256, 2048], P(('ep', 'tp'))
- new_state: float32 [256, 16, 128, 128], P('ep', 'tp')
The draws below stay inside these ranges and needn't reach their ends.
Inputs may be any that keep to these rules, and one draw needn't show every extreme that they name: `expert_ids`: the 4 experts of a row are distinct and lie in one group of 8 consecutive ids. In each aligned block of 16 rows (the rows of one index of ep) no expert is named by more than 8 rows, and at most 16 rows pick one group.
All inputs are finite; a program needn't handle non-finite values.
Results may differ from the reference program's by a relative error of at most 0.012.
Values may be sent and summed in bfloat16 or wider, within the bound.
No kernel may reach another device: no remote copies, remote signals or barrier semaphores. Data moves between devices by JAX's collectives and lax.ppermute only.
A program may use at most 128 MiB of HBM per device.

```python
import math
import jax
import jax.numpy as jnp
from jax import lax

D = 2048
HEADS = 16
HEAD = 128
FFE = 1024
FFD = 4096
EPG = 8
TOP_K = 4
SEQ_GROUP = 16
HD = 2048
EXPERTS = 16
GROUPS = 2
GCAP = 16
CAP = 8
SLOTS = 128
TOKENS = 256


def draw_expert_ids(key, part):
    base = jax.random.fold_in(key, 11)
    key_hot, key_blocks = jax.random.split(base)
    hot_base = jax.random.randint(key_hot, (), 0, GROUPS)
    block_count = TOKENS // SEQ_GROUP

    def one_block(block_key, block_number):
        hot_group = (hot_base + block_number) % GROUPS
        key_pool, key_order, key_labels = jax.random.split(block_key, 3)
        others = (hot_group + 1 + jnp.repeat(jnp.arange(GROUPS - 1, dtype=jnp.int32), GCAP)) % GROUPS
        others = jax.random.permutation(key_pool, others)
        pool = jnp.concatenate([jnp.full((GCAP,), hot_group, jnp.int32), others.astype(jnp.int32)])[:SEQ_GROUP]
        groups = jax.random.permutation(key_order, pool)
        positions = jnp.arange(SEQ_GROUP, dtype=jnp.int32)
        same_group = groups[:, None] == groups[None, :]
        earlier = positions[None, :] < positions[:, None]
        rank_in = jnp.sum((same_group & earlier).astype(jnp.int32), axis=1)
        local = (rank_in[:, None] * TOP_K + jnp.arange(TOP_K, dtype=jnp.int32)[None, :]) % EPG
        labels = jax.vmap(lambda label_key: jax.random.permutation(label_key, EPG))(jax.random.split(key_labels, GROUPS)).astype(jnp.int32)
        chosen = labels[groups[:, None], local]
        return (groups[:, None] * EPG + chosen).astype(jnp.int32)
    blocks = jax.vmap(one_block)(jax.random.split(key_blocks, block_count), jnp.arange(block_count, dtype=jnp.int32))
    return blocks.reshape(TOKENS, TOP_K).astype(jnp.int32)


def shard_levels(key, dims, pieces, smallest, largest):
    level = 1.0
    for position, blocks in pieces:
        draws = jax.random.uniform(jax.random.fold_in(jax.random.fold_in(key, 6), position), (blocks,), jnp.float32, smallest / len(pieces), largest / len(pieces))
        level = level * jnp.repeat(jnp.exp(draws), dims[position] // blocks).reshape((-1,) + (1,) * (len(dims) - 1 - position))
    return level


def bell_draw(key, shape, scale, most, cuts=(), kind=jnp.bfloat16):
    drawn = scale * jax.random.normal(key, shape, jnp.float32)
    if cuts:
        drawn = drawn * shard_levels(key, shape, cuts, -0.22, 0.18)
    return jnp.clip(drawn, -most, most).astype(kind)


def setup_inputs(seed: int = 0) -> dict:
    streams_of = jax.random.split(jax.random.key(seed), 24)
    return {
        "tokens": bell_draw(streams_of[0], (TOKENS, D), 1.0, 6.0, ((0, 32),)),
        "mix_gain": jnp.clip(1.0 + 0.18 * jax.random.normal(streams_of[1], (D,), jnp.float32), 0.1, 1.9),
        "w_query": bell_draw(streams_of[2], (D, HEADS, HEAD), D ** -0.5, 0.125, ((1, 2), (2, 16))),
        "w_key": bell_draw(streams_of[3], (D, HEADS, HEAD), D ** -0.5, 0.125, ((1, 2), (2, 16))),
        "w_value": bell_draw(streams_of[4], (D, HEADS, HEAD), D ** -0.5, 0.125, ((1, 2), (2, 16))),
        "w_zgate": bell_draw(streams_of[5], (D, HEADS, HEAD), D ** -0.5, 0.125, ((1, 2), (2, 16))),
        "w_beta": bell_draw(streams_of[6], (D, HEADS), D ** -0.5, 0.125, ((1, 2),)),
        "w_decay": bell_draw(streams_of[7], (D, HEADS), D ** -0.5, 0.125, ((1, 2),)),
        "decay_rate": jnp.clip(jnp.exp(math.log(8.0) - 2.7725887 * jax.random.uniform(streams_of[8], (HEADS,), jnp.float32) ** shard_levels(streams_of[8], (HEADS,), ((0, 2),), -0.2, 0.2)), 0.5, 8.0),
        "decay_bias": jnp.clip(-3.0 + 3.0 * jax.random.uniform(streams_of[9], (HEADS,), jnp.float32) ** shard_levels(streams_of[9], (HEADS,), ((0, 2),), -0.2, 0.2), -3.0, 0.0),
        "head_gain": jnp.clip(1.0 + 0.18 * jax.random.normal(streams_of[10], (HEAD,), jnp.float32), 0.1, 1.9),
        "state": bell_draw(streams_of[11], (TOKENS, HEADS, HEAD, HEAD), 0.25, 1.5, ((0, 16), (1, 2)), jnp.float32),
        "w_out": bell_draw(streams_of[12], (HD, D), HD ** -0.5, 0.125, ((0, 2), (1, 16))),
        "moe_gain": jnp.clip(1.0 + 0.18 * jax.random.normal(streams_of[13], (D,), jnp.float32), 0.1, 1.9),
        "dense_mix": bell_draw(streams_of[14], (D,), D ** -0.5, 0.125),
        "dense_gate": bell_draw(streams_of[15], (D, FFD), D ** -0.5, 0.125, ((1, 32),)),
        "dense_up": bell_draw(streams_of[16], (D, FFD), D ** -0.5, 0.125, ((1, 32),)),
        "dense_down": bell_draw(streams_of[17], (FFD, D), FFD ** -0.5, 0.09375, ((0, 32),)),
        "expert_gate": bell_draw(streams_of[18], (EXPERTS, D, FFE), D ** -0.5, 0.125, ((0, 16), (2, 2))),
        "expert_up": bell_draw(streams_of[19], (EXPERTS, D, FFE), D ** -0.5, 0.125, ((0, 16), (2, 2))),
        "expert_down": bell_draw(streams_of[20], (EXPERTS, FFE, D), FFE ** -0.5, 0.1875, ((0, 16), (1, 2))),
        "expert_ids": draw_expert_ids(jax.random.fold_in(streams_of[23], 71), 0),
        "route_weight": jnp.clip(jnp.exp(jax.random.uniform(streams_of[22], (TOKENS, TOP_K), jnp.float32, math.log(0.1), math.log(1.0))), 0.1, 1.0),
    }


EPS = 1e-06

def rms_scale(values, gain):
    return values * lax.rsqrt(lax.optimization_barrier(jnp.mean(values * values, axis=-1, keepdims=True)) + EPS) * gain

def unit_rows(values):
    return values * lax.rsqrt(lax.optimization_barrier(jnp.sum(values * values, axis=-1, keepdims=True)) + EPS)

def reference(tokens, mix_gain, w_query, w_key, w_value, w_zgate, w_beta, w_decay, decay_rate, decay_bias, head_gain, state, w_out, moe_gain, dense_mix, dense_gate, dense_up, dense_down, expert_gate, expert_up, expert_down, expert_ids, route_weight):
    tok_float = tokens.astype(jnp.float32)
    normed = rms_scale(tok_float, mix_gain).astype(jnp.bfloat16)

    def project(weight):
        product = jnp.dot(normed, weight.reshape(D, HD), preferred_element_type=jnp.float32)
        return product.astype(jnp.bfloat16).reshape(TOKENS, HEADS, HEAD).astype(jnp.float32)
    query = unit_rows(jax.nn.silu(project(w_query))) * HEAD ** (-0.5)
    key_vec = unit_rows(jax.nn.silu(project(w_key)))
    value = jax.nn.silu(project(w_value))
    gate_in = project(w_zgate)
    beta_rate = jax.nn.sigmoid(jnp.dot(normed, w_beta, preferred_element_type=jnp.float32))
    decay_in = jnp.dot(normed, w_decay, preferred_element_type=jnp.float32)
    retain = jnp.exp(-decay_rate * jax.nn.softplus(decay_in + decay_bias))
    recalled = jnp.einsum('shkv,shk->shv', state, key_vec, precision=lax.Precision.HIGHEST)
    correction = value - retain[..., None] * recalled
    new_state = retain[..., None, None] * state + (beta_rate[..., None] * key_vec)[..., :, None] * correction[..., None, :]
    readout = jnp.einsum('shkv,shk->shv', new_state, query, precision=lax.Precision.HIGHEST)
    gated = rms_scale(readout, head_gain) * jax.nn.silu(gate_in)
    gated = gated.astype(jnp.bfloat16).reshape(TOKENS, HD)
    resid = tok_float + jnp.dot(gated, w_out, preferred_element_type=jnp.float32)
    moe_in = rms_scale(resid, moe_gain).astype(jnp.bfloat16)
    dense_hidden = (jax.nn.silu(jnp.dot(moe_in, dense_gate, preferred_element_type=jnp.float32)) * jnp.dot(moe_in, dense_up, preferred_element_type=jnp.float32)).astype(jnp.bfloat16)
    mix_factor = jax.nn.sigmoid(jnp.dot(moe_in, dense_mix, preferred_element_type=jnp.float32))
    dense_out = mix_factor[:, None] * jnp.dot(dense_hidden, dense_down, preferred_element_type=jnp.float32)
    positions = jnp.arange(TOKENS, dtype=jnp.int32)
    block_idx = positions // SEQ_GROUP
    slot_iota = jnp.arange(SLOTS, dtype=jnp.int32)

    def one_expert(summed, stacked):
        expert, gate_w, up_w, down_w = stacked
        matched = expert_ids == expert
        routed = jnp.any(matched, axis=1).astype(jnp.int32)
        weight = lax.optimization_barrier(jnp.sum(jnp.where(matched, route_weight, 0.0), axis=1))
        rank_in = (jnp.cumsum(routed.reshape(-1, SEQ_GROUP), axis=1).reshape(-1) - routed).astype(jnp.int32)
        slot_idx = (block_idx * CAP + rank_in).astype(jnp.int32)
        matches = (slot_idx[None, :] == slot_iota[:, None]) & (routed[None, :] > 0)
        source = lax.optimization_barrier(jnp.sum(jnp.where(matches, positions[None, :], 0), axis=1)).astype(jnp.int32)
        picked = jnp.take(moe_in, source, axis=0)
        expert_hidden = (jax.nn.silu(jnp.dot(picked, gate_w, preferred_element_type=jnp.float32)) * jnp.dot(picked, up_w, preferred_element_type=jnp.float32)).astype(jnp.bfloat16)
        expert_out = jnp.dot(expert_hidden, down_w, preferred_element_type=jnp.float32)
        row_take = jnp.take(expert_out, jnp.minimum(slot_idx, SLOTS - 1), axis=0)
        return (summed + weight[:, None] * row_take, None)
    moe_out, _ = lax.scan(one_expert, jnp.zeros((TOKENS, D), jnp.float32), (jnp.arange(EXPERTS, dtype=jnp.int32), expert_gate, expert_up, expert_down))
    layer_out = (resid + dense_out + moe_out).astype(jnp.bfloat16)
    return (layer_out, new_state)
```

```python
import functools

import jax
import jax.numpy as jnp
from jax import lax
from jax.experimental import pallas as pl
from jax.experimental.pallas import tpu as pltpu
from jax.sharding import PartitionSpec as P

EPS = 1e-06
AXES = ("ep", "tp")
F32 = jnp.float32
BF16 = jnp.bfloat16
VM = pltpu.VMEM
SM = pltpu.SMEM


def call(kernel, out_shape, operands, scratch=(), smem=(0,), limit=None, grid=None, in_specs=None, out_specs=None, name=None):
    if in_specs is None:
        in_specs = [pl.BlockSpec(memory_space=SM if i in smem else VM) for i in range(len(operands))]
    extra = {} if grid is None else {"grid": grid}
    if out_specs is None:
        out_specs = jax.tree.map(lambda _: pl.BlockSpec(memory_space=VM), out_shape)
    return pl.pallas_call(
        kernel,
        out_shape=out_shape,
        in_specs=in_specs,
        out_specs=out_specs,
        scratch_shapes=list(scratch),
        compiler_params=pltpu.CompilerParams(vmem_limit_bytes=limit),
        name=name,
        **extra,
    )(*operands)


def digits_of(count):
    bits = count.bit_length() - 1
    found = []
    while bits > 0:
        width = 2 if bits >= 2 else 1
        bits -= width
        found.append((bits, 1 << width))
    return found


def masks_of(digits):
    cur = [0]
    for shift, radix in digits[:-1]:
        cur = [(d << shift) | m for d in range(radix) for m in cur]
    shift, radix = digits[-1]
    return [[(d << shift) | m for m in cur] for d in range(radix)]


def exchange(value, mask, swap=0):
    ep_count, tp_count = lax.axis_size("ep"), lax.axis_size("tp")
    pairs = [
        (e * tp_count + t, (e ^ mask) * tp_count + (t ^ swap)) for e in range(ep_count) for t in range(tp_count)
    ]
    return lax.ppermute(value, AXES, pairs)


def gather_xor(piece, digits):
    cur = piece[None]
    for shift, radix in digits[:-1]:
        cur = jnp.concatenate([cur] + [exchange(cur, d << shift) for d in range(1, radix)], axis=0)
    shift, radix = digits[-1]
    return [cur] + [exchange(cur, d << shift) for d in range(1, radix)]


def scale_rows(values, gain):
    return values * lax.rsqrt(jnp.mean(values * values, axis=-1, keepdims=True) + EPS) * gain


def norm_kernel(masks, where, *refs):
    pieces, gain, out = refs[: len(masks)], refs[-2], refs[-1]
    me = where[0]
    for ref, row in zip(pieces, masks):
        for j, mask in enumerate(row):
            out[me ^ mask] = scale_rows(ref[j].astype(F32), gain[...]).astype(BF16)


def project_kernel(where, own, other, wq, wk, wv, wz, out, stacked):
    par = where[1]
    rows, each = wq.shape[0], own.shape[1]
    for p, ref in enumerate((wq, wk, wv, wz)):
        stacked[p * rows : (p + 1) * rows, :] = ref[...]
    for side, ref in ((par, own), (1 - par, other)):
        x = ref[...].reshape(-1, ref.shape[2])
        y = lax.dot_general(x, stacked[...], (((1,), (1,)), ((), ())), preferred_element_type=F32)
        out[:, side] = y.reshape(ref.shape[0], each, -1).astype(BF16)


def rates_kernel(where, own, other, wb, wd, rate, bias, beta, retain):
    me, par = where[0], where[1]
    each = own.shape[1]
    for side, ref in ((par, own), (1 - par, other)):
        x = ref[me]
        b = lax.dot_general(x, wb[...], (((1,), (1,)), ((), ())), preferred_element_type=F32)
        d = lax.dot_general(x, wd[...], (((1,), (1,)), ((), ())), preferred_element_type=F32)
        d = d + bias[...]
        soft = jnp.maximum(d, 0.0) + jnp.log1p(jnp.exp(-jnp.abs(d)))
        beta[side] = 1.0 / (1.0 + jnp.exp(-b))
        retain[side] = jnp.exp(-rate[...] * soft)


def silu(x):
    return x / (1.0 + jnp.exp(-x))


def state_kernel(heads, beta, retain, cols, gain, state, gated, new_state, rows, qt, kt, reads):
    step = pl.program_id(0)
    seqs = pl.num_programs(0)
    size = state.shape[3]

    @pl.when(step == 0)
    def _():
        table = cols[...]
        width = table.shape[1]
        count = table.shape[0] // gated.shape[0]
        piece = width // (4 * heads)
        lane = lax.broadcasted_iota(jnp.int32, (table.shape[0], size), 1)
        src = lax.broadcasted_iota(jnp.int32, (table.shape[0], size), 0)
        keep = (lane // piece) == (src // gated.shape[0])
        pick_lane = lax.broadcasted_iota(jnp.int32, (width, size), 1) % piece
        pick_row = lax.broadcasted_iota(jnp.int32, (width, size), 0)
        for p in range(4):
            for h in range(heads):
                pick = jnp.where(pick_row == pick_lane + (p * heads + h) * piece, 1.0, 0.0).astype(BF16)
                spread = jnp.dot(table, pick, preferred_element_type=F32)
                spread = jnp.where(keep, spread, 0.0).reshape(count, gated.shape[0], size)
                rows[p, pl.ds(h, gated.shape[0], stride=heads), :] = jnp.sum(spread, axis=0)
        q = silu(rows[0])
        q = q * lax.rsqrt(jnp.sum(q * q, axis=-1, keepdims=True) + EPS) * size ** (-0.5)
        qt[...] = q.T
        k = silu(rows[1])
        k = k * lax.rsqrt(jnp.sum(k * k, axis=-1, keepdims=True) + EPS)
        kt[...] = k.T
        rows[2] = silu(rows[2])
        rows[3] = silu(rows[3])

    lanes = qt.shape[1]
    back = lax.rem(lanes - step * heads, lanes)
    q_cols = pltpu.roll(qt[...], back, 1)
    k_cols = pltpu.roll(kt[...], back, 1)
    first = pl.multiple_of(step * heads, heads)
    values = rows[2, pl.ds(first, heads), :]
    gates = rows[3, pl.ds(first, heads), :]
    found = []
    for h in range(heads):
        keep_rate = retain[step, h]
        write_rate = beta[step, h]
        old = state[0, h]
        k_wide = jnp.broadcast_to(k_cols[:, h : h + 1], (size, size))
        q_wide = jnp.broadcast_to(q_cols[:, h : h + 1], (size, size))
        recalled = jnp.sum(old * k_wide, axis=0, keepdims=True)
        change = write_rate * (values[h : h + 1, :] - keep_rate * recalled)
        new = keep_rate * old + k_wide * change
        new_state[0, h] = new
        found.append(jnp.sum(new * q_wide, axis=0, keepdims=True))
    read = jnp.concatenate(found, axis=0)
    reads[pl.ds(first, heads), :] = scale_rows(read, gain[...]) * gates

    @pl.when(step == seqs - 1)
    def _():
        for h in range(heads):
            gated[:, h * size : (h + 1) * size] = reads[pl.ds(h, gated.shape[0], stride=heads), :].astype(BF16)


def mix_kernel(masks, where, *refs):
    pieces, weight, out = refs[: len(masks)], refs[-2], refs[-1]
    me, par = where[0], where[1]
    each = out.shape[2]
    for ref, row in zip(pieces, masks):
        x = ref[...].reshape(-1, ref.shape[2])
        y = jnp.dot(x, weight[...], preferred_element_type=F32)
        y = y.reshape(len(row), 2, each, -1).astype(BF16)
        for j, mask in enumerate(row):
            for side in range(2):
                out[side ^ par, me ^ mask] = y[j, side]


def resid_kernel(masks, where, *refs):
    count = len(masks)
    tokens, mixed, gain = refs[:count], refs[count:-4], refs[-4]
    moe, own, resid = refs[-3:]
    me = where[0]
    each = own.shape[0]
    for ref, row in zip(tokens, masks):
        for j, mask in enumerate(row):
            at = pl.multiple_of((me ^ mask) * each, each)
            resid[pl.ds(at, each), :] = ref[j].astype(F32)
    if len(mixed) == 1:
        resid[...] = resid[...] + mixed[0][...].astype(F32)
    for ref, row in zip(mixed, masks if len(mixed) > 1 else ()):
        for j, mask in enumerate(row):
            width = ref.shape[2]
            at = pl.ds(pl.multiple_of((me ^ mask) * width, width), width)
            resid[:, at] = resid[:, at] + ref[j].astype(F32)
    moe[...] = scale_rows(resid[...], gain[...]).astype(BF16)
    own[...] = resid[pl.ds(pl.multiple_of(me * each, each), each), :]


def expert_kernel(rows_in, route, mix, d_gate, d_up, d_down, e_gate, e_up, e_down, out):
    x = rows_in[...]
    dot = functools.partial(jnp.dot, preferred_element_type=F32)
    hidden = (silu(dot(x, e_gate[...])) * dot(x, e_up[...])).astype(BF16)
    dense = (silu(dot(x, d_gate[...])) * dot(x, d_up[...])).astype(BF16)
    factor = jnp.sum(x.astype(F32) * mix[...].astype(F32), axis=1, keepdims=True)
    factor = 1.0 / (1.0 + jnp.exp(-factor))
    out[...] = (route[...] * dot(hidden, e_down[...]) + factor * dot(dense, d_down[...])).astype(out.dtype)


def fold_kernel(masks, where, own, other, *outs):
    me = where[0]
    each = outs[0].shape[1]
    for out, row in zip(outs, masks):
        for j, mask in enumerate(row):
            at = pl.ds(pl.multiple_of((me ^ mask) * each, each), each)
            out[j] = (own[at, :].astype(F32) + other[at, :].astype(F32)).astype(BF16)


def sum_kernel(parts, *refs):
    outs = refs[parts:]
    for i, out in enumerate(outs):
        total = refs[0][i].astype(F32)
        for ref in refs[1:parts]:
            total = total + ref[i].astype(F32)
        out[...] = total.astype(out.dtype)


def last_kernel(resid, *refs):
    total = refs[0][...].astype(F32)
    for ref in refs[1:-1]:
        total = total + ref[...].astype(F32)
    refs[-1][...] = (resid[...] + total).astype(refs[-1].dtype)


def body(
    tokens,
    mix_gain,
    w_query,
    w_key,
    w_value,
    w_zgate,
    w_beta,
    w_decay,
    decay_rate,
    decay_bias,
    head_gain,
    state,
    w_out,
    moe_gain,
    dense_mix,
    dense_gate,
    dense_up,
    dense_down,
    expert_gate,
    expert_up,
    expert_down,
    expert_ids,
    route_weight,
):
    ep_count = lax.axis_size("ep")
    me, par = lax.axis_index("ep"), lax.axis_index("tp")
    where = jnp.stack([me, par]).astype(jnp.int32)
    digits = digits_of(ep_count)
    masks = masks_of(digits)
    each, width = tokens.shape
    seqs, heads, size = state.shape[:3]
    half = ep_count * each
    sds = jax.ShapeDtypeStruct

    tok_pieces = gather_xor(tokens, digits)
    normed = call(
        functools.partial(norm_kernel, masks),
        sds((ep_count, each, width), BF16),
        [where, *tok_pieces, mix_gain[None]],
        name="norm",
    )
    normed_other = exchange(normed, 0, 1)

    flat = [w.transpose(1, 2, 0).reshape(-1, width) for w in (w_query, w_key, w_value, w_zgate)]
    columns = 4 * flat[0].shape[0]
    projected = call(
        project_kernel,
        sds((ep_count, 2, each, columns), BF16),
        [where, normed, normed_other, *flat],
        scratch=[VM((columns, width), BF16)],
        name="project",
    )
    by_seq = lax.all_to_all(projected, "ep", split_axis=0, concat_axis=0, tiled=True)
    beta, retain = call(
        rates_kernel,
        (sds((2, each, heads), F32), sds((2, each, heads), F32)),
        [where, normed, normed_other, w_beta.T, w_decay.T, decay_rate[None], decay_bias[None]],
        name="rates",
    )

    whole = lambda shape: pl.BlockSpec(shape, lambda i: (0,) * len(shape))
    blocked = pl.BlockSpec((1, heads, size, size), lambda i: (i, 0, 0, 0))
    gated, new_state = call(
        functools.partial(state_kernel, heads),
        (sds((seqs, heads * size), BF16), sds(state.shape, F32)),
        [
            beta.reshape(seqs, heads),
            retain.reshape(seqs, heads),
            by_seq.reshape(ep_count * seqs, columns),
            head_gain[None],
            state,
        ],
        scratch=[
            VM((4, seqs * heads, size), F32),
            VM((size, seqs * heads), F32),
            VM((size, seqs * heads), F32),
            VM((seqs * heads, size), F32),
        ],
        grid=(seqs,),
        in_specs=[
            pl.BlockSpec(memory_space=SM),
            pl.BlockSpec(memory_space=SM),
            whole((ep_count * seqs, columns)),
            whole((1, size)),
            blocked,
        ],
        out_specs=(whole((seqs, heads * size)), blocked),
        name="state",
    )

    gated_pieces = gather_xor(gated, digits)
    out_cols = w_out.shape[1]
    mixed = call(
        functools.partial(mix_kernel, masks),
        sds((2, ep_count, each, out_cols), BF16),
        [where, *gated_pieces, w_out],
        name="mix",
    )
    mixed = (mixed[0].astype(F32) + exchange(mixed[1], 0, 1).astype(F32)).astype(BF16).reshape(half, out_cols)
    mixed_pieces = gather_xor(mixed, digits)
    if out_cols % 128:
        order = jnp.argsort(me ^ jnp.array([m for row in masks for m in row], jnp.int32))
        blocks = jnp.take(jnp.concatenate(mixed_pieces, axis=0), order, axis=0)
        mixed_pieces = [blocks.transpose(1, 0, 2).reshape(half, width)]
    moe_in, resid = call(
        functools.partial(resid_kernel, masks),
        (sds((half, width), BF16), sds((each, width), F32)),
        [where, *tok_pieces, *mixed_pieces, moe_gain[None]],
        scratch=[VM((half, width), F32)],
        name="resid",
    )
    moe_other = exchange(moe_in, 0, 1)

    chosen = jnp.sum(jnp.where(expert_ids == me, route_weight, 0.0), axis=1).reshape(ep_count, 2, each)
    route = lax.dynamic_index_in_dim(chosen, par, 1, False).reshape(half, 1)
    route_other = lax.dynamic_index_in_dim(chosen, 1 - par, 1, False).reshape(half, 1)
    weights = [dense_mix[None], dense_gate, dense_up, dense_down, expert_gate[0], expert_up[0], expert_down[0]]
    run = lambda x, r, dt, name: call(expert_kernel, sds((half, width), dt), [x, r, *weights], smem=(), name=name)
    part_own = run(moe_in, route, F32, "experts_own")
    part_other = run(moe_other, route_other, BF16, "experts_other")

    prev = len(masks[0])
    parts = call(
        functools.partial(fold_kernel, masks),
        tuple(sds((prev, each, width), BF16) for _ in masks),
        [where, part_own, exchange(part_other, 0, 1)],
        name="fold",
    )
    for level in range(len(digits) - 1, 0, -1):
        shift, radix = digits[level]
        got = [parts[0]] + [exchange(parts[d], d << shift) for d in range(1, radix)]
        nxt = digits[level - 1][1]
        got = [g.reshape(nxt, -1, width) for g in got]
        parts = call(
            functools.partial(sum_kernel, len(got)),
            tuple(sds(got[0].shape[1:], BF16) for _ in range(nxt)),
            got,
            smem=(),
            name=f"sum{level}",
        )
    shift, radix = digits[0]
    got = [parts[0]] + [exchange(parts[d], d << shift) for d in range(1, radix)]
    layer_out = call(last_kernel, sds((each, width), BF16), [resid, *got], smem=(), name="last")
    return (layer_out, new_state)


def solution(mesh):
    placed = (
        P(("ep", "tp"), None),
        P(),
        P(None, "tp", "ep"),
        P(None, "tp", "ep"),
        P(None, "tp", "ep"),
        P(None, "tp", "ep"),
        P(None, "tp"),
        P(None, "tp"),
        P("tp"),
        P("tp"),
        P(),
        P("ep", "tp", None, None),
        P("tp", "ep"),
        P(),
        P(),
        P(None, ("ep", "tp")),
        P(None, ("ep", "tp")),
        P(("ep", "tp"), None),
        P("ep", None, "tp"),
        P("ep", None, "tp"),
        P("ep", "tp", None),
        P(),
        P(),
    )
    return jax.shard_map(
        body,
        mesh=mesh,
        in_specs=placed,
        out_specs=(P(("ep", "tp"), None), P("ep", "tp", None, None)),
        check_vma=False,
    )
```

```python
import functools

import jax
import jax.numpy as jnp
from jax import lax
from jax.experimental import pallas as pl
from jax.experimental.pallas import tpu as pltpu
from jax.sharding import PartitionSpec as P

EPS = 1e-06
AXES = ("ep", "tp")
F32 = jnp.float32
BF16 = jnp.bfloat16
VM = pltpu.VMEM
SM = pltpu.SMEM


def padded_bytes(shape, dtype):
    shape = (1, 1) + tuple(shape)
    item = jnp.dtype(dtype).itemsize
    lead = 1
    for n in shape[:-2]:
        lead *= n
    return lead * -(-shape[-2] // 8) * 8 * -(-shape[-1] // 128) * 128 * item


def call(kernel, out_shape, operands, scratch=(), smem=(0,), hbm=(), loose=(), hbm_out=(), spare=2, name=None):
    outs, tree = jax.tree.flatten(out_shape)
    held = [x for i, x in enumerate(operands) if i not in smem and i not in hbm and i not in loose]
    held += [x for i, x in enumerate(outs) if i not in hbm_out]
    held += [x for x in scratch if hasattr(x, "shape") and getattr(x, "memory_space", None) == VM]
    limit = sum(padded_bytes(x.shape, x.dtype) for x in held) + (spare << 20)
    space = lambda i: SM if i in smem else pltpu.HBM if i in hbm else pl.ANY if i in loose else VM
    return pl.pallas_call(
        kernel,
        out_shape=out_shape,
        in_specs=[pl.BlockSpec(memory_space=space(i)) for i in range(len(operands))],
        out_specs=jax.tree.unflatten(
            tree, [pl.BlockSpec(memory_space=pltpu.HBM if i in hbm_out else VM) for i in range(len(outs))]
        ),
        scratch_shapes=list(scratch),
        compiler_params=pltpu.CompilerParams(vmem_limit_bytes=limit),
        name=name,
    )(*[pltpu.with_memory_space_constraint(x, pltpu.HBM) if i in hbm else x for i, x in enumerate(operands)])


def digits_of(count):
    bits = count.bit_length() - 1
    found = []
    while bits > 0:
        width = 2 if bits >= 2 else 1
        bits -= width
        found.append((bits, 1 << width))
    return found


def masks_of(digits):
    cur = [0]
    for shift, radix in digits[:-1]:
        cur = [(d << shift) | m for d in range(radix) for m in cur]
    shift, radix = digits[-1]
    return [[(d << shift) | m for m in cur] for d in range(radix)]


def exchange(value, mask, swap=0):
    ep_count, tp_count = lax.axis_size("ep"), lax.axis_size("tp")
    pairs = [
        (e * tp_count + t, (e ^ mask) * tp_count + (t ^ swap)) for e in range(ep_count) for t in range(tp_count)
    ]
    return lax.ppermute(value, AXES, pairs)


def gather_xor(piece, digits):
    cur = piece[None]
    for shift, radix in digits[:-1]:
        cur = jnp.concatenate([cur] + [exchange(cur, d << shift) for d in range(1, radix)], axis=0)
    shift, radix = digits[-1]
    return [cur] + [exchange(cur, d << shift) for d in range(1, radix)]


def scale_rows(values, gain):
    return values * lax.rsqrt(jnp.mean(values * values, axis=-1, keepdims=True) + EPS) * gain


def load_kernel(after, wq, wk, wv, wz, gain, stacked, gain_out, rows, sems):
    each = wq.shape[0]
    copies = [
        pltpu.make_async_copy(ref, rows.at[pl.ds(p * each, each), :], sems.at[p]) for p, ref in enumerate((wq, wk, wv, wz))
    ]
    copies.append(pltpu.make_async_copy(gain, gain_out, sems.at[4]))
    for c in copies:
        c.start()
    for c in copies:
        c.wait()
    stacked[...] = rows[...].astype(F32).T.astype(BF16)


def norm_kernel(masks, where, *refs):
    pieces, gain, out = refs[: len(masks)], refs[-3], refs[-1]
    me = where[0]
    for ref, row in zip(pieces, masks):
        for j, mask in enumerate(row):
            out[me ^ mask] = scale_rows(ref[j].astype(F32), gain[...]).astype(BF16)


def project_kernel(other, where, x_ref, stacked, *refs):
    out = refs[-1]
    side = 1 - where[1] if other else where[1]
    x = x_ref[...].reshape(-1, x_ref.shape[2])
    y = jnp.dot(x, stacked[...], preferred_element_type=F32)
    out[:, side] = y.reshape(out.shape[0], out.shape[2], -1).astype(BF16)
    if other:
        out[:, 1 - side] = refs[0][:, 1 - side]


def rates_kernel(where, own, other, wb, wd, rate, bias, ids, chance, beta, retain, route, route_other, column):
    me, par = where[0], where[1]
    each = own.shape[1]
    for side, ref in ((par, own), (1 - par, other)):
        x = ref[me]
        b = lax.dot_general(x, wb[...], (((1,), (1,)), ((), ())), preferred_element_type=F32)
        d = lax.dot_general(x, wd[...], (((1,), (1,)), ((), ())), preferred_element_type=F32)
        d = d + bias[...]
        soft = jnp.maximum(d, 0.0) + jnp.log1p(jnp.exp(-jnp.abs(d)))
        beta[side] = 1.0 / (1.0 + jnp.exp(-b))
        retain[side] = jnp.exp(-rate[...] * soft)
    picked = jnp.sum(jnp.where(ids[...] == me, chance[...], 0.0), axis=0, keepdims=True)
    picked = jnp.broadcast_to(picked, (8, picked.shape[1])).T[:, :1]
    column[...] = picked.reshape(column.shape)
    route[...] = column[:, par].reshape(route.shape)
    route_other[...] = column[:, 1 - par].reshape(route.shape)


def silu(x):
    return x / (1.0 + jnp.exp(-x))


def regroup(blocks, piece):
    lane = lax.broadcasted_iota(jnp.int32, blocks[0].shape, 1) // piece
    step = 1
    while step < len(blocks):
        low = (lane & step) == 0
        blocks = list(blocks)
        for i in range(len(blocks)):
            if i & step:
                continue
            a, b = blocks[i], blocks[i | step]
            lanes = a.shape[1]
            blocks[i] = jnp.where(low, a, pltpu.roll(b, step * piece, 1))
            blocks[i | step] = jnp.where(low, pltpu.roll(a, lanes - step * piece, 1), b)
        step *= 2
    return blocks


def state_kernel(
    heads, cols, beta, retain, gain, state, gated, new_state, rows, qt, kt, reads, old, new, wide, sem_in, sem_out
):
    seqs, size = state.shape[0], state.shape[3]
    fetch = lambda i: pltpu.make_async_copy(state.at[i], old.at[i], sem_in.at[i])
    store = lambda i: pltpu.make_async_copy(new.at[i], new_state.at[i], sem_out.at[i])
    for i in range(seqs):
        fetch(i).start()
    count, width = cols.shape[0], cols.shape[2]
    piece = width // (4 * heads)
    for first in range(0, width, size):
        blocks = []
        for e in range(count):
            block = cols[e, :, first : min(first + size, width)].astype(F32)
            if block.shape[1] < size:
                block = jnp.concatenate([block, jnp.zeros((seqs, size - block.shape[1]), F32)], axis=1)
            blocks.append(block)
        for i, block in enumerate(regroup(blocks, piece)):
            n = first // piece + i
            if n < 4 * heads:
                rows[n // heads, pl.ds(n % heads, seqs, stride=heads), :] = block
    for h in range(heads):
        rows[4, pl.ds(h, seqs, stride=heads), :] = jnp.broadcast_to(beta[:, h : h + 1], (seqs, size))
        rows[5, pl.ds(h, seqs, stride=heads), :] = jnp.broadcast_to(retain[:, h : h + 1], (seqs, size))
    q = silu(rows[0])
    q = q * lax.rsqrt(jnp.sum(q * q, axis=-1, keepdims=True) + EPS) * size ** (-0.5)
    qt[...] = q.T
    k = silu(rows[1])
    k = k * lax.rsqrt(jnp.sum(k * k, axis=-1, keepdims=True) + EPS)
    kt[...] = k.T
    rows[6] = jnp.broadcast_to(jnp.sum(q * k, axis=-1, keepdims=True), k.shape)
    rows[2] = silu(rows[2])
    rows[3] = silu(rows[3])
    lanes = qt.shape[1]

    def one(step, carry):
        fetch(step).wait()
        back = lax.rem(lanes - step * heads, lanes)
        q_cols = pltpu.roll(qt[...], back, 1)
        k_cols = pltpu.roll(kt[...], back, 1)
        at = pl.ds(pl.multiple_of(step * heads, heads), heads)
        by_key, by_query = [], []
        for h in range(heads):
            key_sum = query_sum = None
            for i in range(0, size, 8):
                part = old[step, h, i : i + 8, :]
                k_wide = jnp.broadcast_to(k_cols[i : i + 8, h : h + 1], (8, size))
                q_wide = jnp.broadcast_to(q_cols[i : i + 8, h : h + 1], (8, size))
                wide[h, i : i + 8, :] = k_wide
                key_sum = part * k_wide if key_sum is None else key_sum + part * k_wide
                query_sum = part * q_wide if query_sum is None else query_sum + part * q_wide
            by_key.append(jnp.sum(key_sum, axis=0, keepdims=True))
            by_query.append(jnp.sum(query_sum, axis=0, keepdims=True))
        keep = rows[5, at, :]
        change = rows[4, at, :] * (rows[2, at, :] - keep * jnp.concatenate(by_key, axis=0))
        read = keep * jnp.concatenate(by_query, axis=0) + rows[6, at, :] * change
        for h in range(heads):
            keep_h = jnp.broadcast_to(keep[h : h + 1, :], (8, size))
            change_h = jnp.broadcast_to(change[h : h + 1, :], (8, size))
            for i in range(0, size, 8):
                new[step, h, i : i + 8, :] = keep_h * old[step, h, i : i + 8, :] + wide[h, i : i + 8, :] * change_h
        store(step).start()
        reads[at, :] = scale_rows(read, gain[...]) * rows[3, at, :]
        return carry

    lax.fori_loop(0, seqs, one, 0)
    for h in range(heads):
        gated[:, h * size : (h + 1) * size] = reads[pl.ds(h, seqs, stride=heads), :].astype(BF16)
    for i in range(seqs):
        store(i).wait()


def mix_kernel(masks, where, *refs):
    pieces, weight, out, out_other, both = refs[: len(masks)], *refs[-4:]
    me, par = where[0], where[1]
    each = out.shape[1]
    for ref, row in zip(pieces, masks):
        x = ref[...].reshape(-1, ref.shape[2])
        y = jnp.dot(x, weight[...], preferred_element_type=F32)
        y = y.reshape(len(row), 2, each, -1).astype(BF16)
        for j, mask in enumerate(row):
            for side in range(2):
                both[side, me ^ mask] = y[j, side]
    out[...] = both[par]
    out_other[...] = both[1 - par]


def pair_kernel(own, other, out):
    out[...] = (own[...].astype(F32) + other[...].astype(F32)).reshape(out.shape).astype(out.dtype)


def resid_kernel(masks, where, *refs):
    count = len(masks)
    tokens, mixed, gain = refs[:count], refs[count:-4], refs[-4]
    moe, own, resid = refs[-3:]
    me = where[0]
    each = own.shape[0]
    for ref, row in zip(tokens, masks):
        for j, mask in enumerate(row):
            at = pl.multiple_of((me ^ mask) * each, each)
            resid[pl.ds(at, each), :] = ref[j].astype(F32)
    if len(mixed) == 1:
        resid[...] = resid[...] + mixed[0][...].astype(F32)
    for ref, row in zip(mixed, masks if len(mixed) > 1 else ()):
        for j, mask in enumerate(row):
            width = ref.shape[2]
            at = pl.ds(pl.multiple_of((me ^ mask) * width, width), width)
            resid[:, at] = resid[:, at] + ref[j].astype(F32)
    moe[...] = scale_rows(resid[...], gain[...]).astype(BF16)
    own[...] = resid[pl.ds(pl.multiple_of(me * each, each), each), :]


def expert_kernel(rows_in, route, mix, d_gate, d_up, d_down, e_gate, e_up, e_down, out):
    x = rows_in[...]
    dot = functools.partial(jnp.dot, preferred_element_type=F32)
    hidden = (silu(dot(x, e_gate[...])) * dot(x, e_up[...])).astype(BF16)
    dense = (silu(dot(x, d_gate[...])) * dot(x, d_up[...])).astype(BF16)
    factor = jnp.sum(x.astype(F32) * mix[...].astype(F32), axis=1, keepdims=True)
    factor = 1.0 / (1.0 + jnp.exp(-factor))
    out[...] = (route[...] * dot(hidden, e_down[...]) + factor * dot(dense, d_down[...])).astype(out.dtype)


def fold_kernel(masks, where, own, other, *outs):
    me = where[0]
    each = outs[0].shape[1]
    for out, row in zip(outs, masks):
        for j, mask in enumerate(row):
            at = pl.ds(pl.multiple_of((me ^ mask) * each, each), each)
            out[j] = (own[at, :].astype(F32) + other[at, :].astype(F32)).astype(BF16)


def sum_kernel(parts, *refs):
    outs = refs[parts:]
    for i, out in enumerate(outs):
        total = refs[0][i].astype(F32)
        for ref in refs[1:parts]:
            total = total + ref[i].astype(F32)
        out[...] = total.astype(out.dtype)


def last_kernel(resid, *refs):
    total = refs[0][...].astype(F32)
    for ref in refs[1:-1]:
        total = total + ref[...].astype(F32)
    refs[-1][...] = (resid[...] + total).astype(refs[-1].dtype)


def body(
    tokens,
    mix_gain,
    w_query,
    w_key,
    w_value,
    w_zgate,
    w_beta,
    w_decay,
    decay_rate,
    decay_bias,
    head_gain,
    state,
    w_out,
    moe_gain,
    dense_mix,
    dense_gate,
    dense_up,
    dense_down,
    expert_gate,
    expert_up,
    expert_down,
    expert_ids,
    route_weight,
):
    ep_count = lax.axis_size("ep")
    me, par = lax.axis_index("ep"), lax.axis_index("tp")
    where = jnp.stack([me, par]).astype(jnp.int32)
    digits = digits_of(ep_count)
    masks = masks_of(digits)
    each, width = tokens.shape
    seqs, heads, size = state.shape[:3]
    half = ep_count * each
    sds = jax.ShapeDtypeStruct

    flat = [w.transpose(1, 2, 0).reshape(-1, width) for w in (w_query, w_key, w_value, w_zgate)]
    columns = 4 * flat[0].shape[0]
    tok_pieces = gather_xor(tokens, digits)
    stacked, gain_near = call(
        load_kernel,
        (sds((width, columns), BF16), sds((1, width), F32)),
        [tok_pieces[0], *flat, mix_gain[None]],
        scratch=[VM((columns, width), BF16), pltpu.SemaphoreType.DMA((5,))],
        smem=(),
        hbm=range(1, 6),
        loose=(0,),
        spare=6,
        name="load",
    )
    normed = call(
        functools.partial(norm_kernel, masks),
        sds((ep_count, each, width), BF16),
        [where, *tok_pieces, gain_near, stacked],
        loose=(len(masks) + 2,),
        name="norm",
    )
    normed_other = exchange(normed, 0, 1)
    shape = sds((ep_count, 2, each, columns), BF16)
    projected = call(
        functools.partial(project_kernel, False), shape, [where, normed, stacked], spare=3, name="project_own"
    )
    projected = call(
        functools.partial(project_kernel, True),
        shape,
        [where, normed_other, stacked, projected],
        spare=3,
        name="project_other",
    )
    by_seq = lax.all_to_all(projected, "ep", split_axis=0, concat_axis=0, tiled=True)
    beta, retain, route, route_other = call(
        rates_kernel,
        (
            sds((2, each, heads), F32),
            sds((2, each, heads), F32),
            sds((half, 1), F32),
            sds((half, 1), F32),
        ),
        [
            where,
            normed,
            normed_other,
            w_beta.T,
            w_decay.T,
            decay_rate[None],
            decay_bias[None],
            expert_ids.T,
            route_weight.T,
        ],
        scratch=[VM((ep_count, 2, each, 1), F32)],
        name="rates",
    )

    gated, new_state = call(
        functools.partial(state_kernel, heads),
        (sds((seqs, heads * size), BF16), sds(state.shape, F32)),
        [
            by_seq.reshape(ep_count, seqs, columns),
            beta.reshape(seqs, heads),
            retain.reshape(seqs, heads),
            head_gain[None],
            state,
        ],
        smem=(),
        hbm=(4,),
        hbm_out=(1,),
        scratch=[
            VM((7, seqs * heads, size), F32),
            VM((size, seqs * heads), F32),
            VM((size, seqs * heads), F32),
            VM((seqs * heads, size), F32),
            VM(state.shape, F32),
            VM(state.shape, F32),
            VM((heads, size, size), F32),
            pltpu.SemaphoreType.DMA((seqs,)),
            pltpu.SemaphoreType.DMA((seqs,)),
        ],
        name="state",
    )

    gated_pieces = gather_xor(gated, digits)
    out_cols = w_out.shape[1]
    mixed, mixed_other = call(
        functools.partial(mix_kernel, masks),
        (sds((ep_count, each, out_cols), BF16), sds((ep_count, each, out_cols), BF16)),
        [where, *gated_pieces, w_out],
        scratch=[VM((2, ep_count, each, out_cols), BF16)],
        name="mix",
    )
    mixed_other = exchange(mixed_other, 0, 1)
    mixed = call(pair_kernel, sds((half, out_cols), BF16), [mixed, mixed_other], smem=(), name="pair")
    mixed_pieces = gather_xor(mixed, digits)
    if out_cols % 128:
        order = jnp.argsort(me ^ jnp.array([m for row in masks for m in row], jnp.int32))
        blocks = jnp.take(jnp.concatenate(mixed_pieces, axis=0), order, axis=0)
        mixed_pieces = [blocks.transpose(1, 0, 2).reshape(half, width)]
    moe_in, resid = call(
        functools.partial(resid_kernel, masks),
        (sds((half, width), BF16), sds((each, width), F32)),
        [where, *tok_pieces, *mixed_pieces, moe_gain[None]],
        scratch=[VM((half, width), F32)],
        name="resid",
    )
    moe_other = exchange(moe_in, 0, 1)

    weights = [dense_mix[None], dense_gate, dense_up, dense_down, expert_gate[0], expert_up[0], expert_down[0]]
    run = lambda x, r, dt, name: call(expert_kernel, sds((half, width), dt), [x, r, *weights], smem=(), spare=6, name=name)
    part_own = run(moe_in, route, F32, "experts_own")
    part_other = run(moe_other, route_other, BF16, "experts_other")

    prev = len(masks[0])
    parts = call(
        functools.partial(fold_kernel, masks),
        tuple(sds((prev, each, width), BF16) for _ in masks),
        [where, part_own, exchange(part_other, 0, 1)],
        name="fold",
    )
    for level in range(len(digits) - 1, 0, -1):
        shift, radix = digits[level]
        got = [parts[0]] + [exchange(parts[d], d << shift) for d in range(1, radix)]
        nxt = digits[level - 1][1]
        got = [g.reshape(nxt, -1, width) for g in got]
        parts = call(
            functools.partial(sum_kernel, len(got)),
            tuple(sds(got[0].shape[1:], BF16) for _ in range(nxt)),
            got,
            smem=(),
            name=f"sum{level}",
        )
    shift, radix = digits[0]
    got = [parts[0]] + [exchange(parts[d], d << shift) for d in range(1, radix)]
    layer_out = call(last_kernel, sds((each, width), BF16), [resid, *got], smem=(), name="last")
    return (layer_out, new_state)


def solution(mesh):
    placed = (
        P(("ep", "tp"), None),
        P(),
        P(None, "tp", "ep"),
        P(None, "tp", "ep"),
        P(None, "tp", "ep"),
        P(None, "tp", "ep"),
        P(None, "tp"),
        P(None, "tp"),
        P("tp"),
        P("tp"),
        P(),
        P("ep", "tp", None, None),
        P("tp", "ep"),
        P(),
        P(),
        P(None, ("ep", "tp")),
        P(None, ("ep", "tp")),
        P(("ep", "tp"), None),
        P("ep", None, "tp"),
        P("ep", None, "tp"),
        P("ep", "tp", None),
        P(),
        P(),
    )
    return jax.shard_map(
        body,
        mesh=mesh,
        in_specs=placed,
        out_specs=(P(("ep", "tp"), None), P("ep", "tp", None, None)),
        check_vma=False,
    )
```

```python
import functools

import jax
import jax.numpy as jnp
from jax import lax
from jax.experimental import pallas as pl
from jax.experimental.pallas import tpu as pltpu
from jax.sharding import PartitionSpec as P


EPS = 1e-06
AXES = ("ep", "tp")
F32 = jnp.float32
BF16 = jnp.bfloat16
VM = pltpu.VMEM
SM = pltpu.SMEM


def padded_bytes(shape, dtype):
    shape = (1, 1) + tuple(shape)
    item = jnp.dtype(dtype).itemsize
    lead = 1
    for n in shape[:-2]:
        lead *= n
    return lead * -(-shape[-2] // 8) * 8 * -(-shape[-1] // 128) * 128 * item


def call(kernel, out_shape, operands, scratch=(), smem=(0,), hbm=(), loose=(), hbm_out=(), spare=2):
    outs, tree = jax.tree.flatten(out_shape)
    held = [x for i, x in enumerate(operands) if i not in smem and i not in hbm and i not in loose]
    held += [x for i, x in enumerate(outs) if i not in hbm_out]
    held += [x for x in scratch if hasattr(x, "shape") and getattr(x, "memory_space", None) == VM]
    limit = sum(padded_bytes(x.shape, x.dtype) for x in held) + (spare << 20)
    space = lambda i: SM if i in smem else pltpu.HBM if i in hbm else pl.ANY if i in loose else VM
    return pl.pallas_call(
        kernel,
        out_shape=out_shape,
        in_specs=[pl.BlockSpec(memory_space=space(i)) for i in range(len(operands))],
        out_specs=jax.tree.unflatten(
            tree, [pl.BlockSpec(memory_space=pltpu.HBM if i in hbm_out else VM) for i in range(len(outs))]
        ),
        scratch_shapes=list(scratch),
        compiler_params=pltpu.CompilerParams(vmem_limit_bytes=limit),
    )(*[pltpu.with_memory_space_constraint(x, pltpu.HBM) if i in hbm else x for i, x in enumerate(operands)])


def digits_of(count):
    bits = count.bit_length() - 1
    found = []
    while bits > 0:
        width = 2 if bits >= 2 else 1
        bits -= width
        found.append((bits, 1 << width))
    return found


def masks_of(digits):
    cur = [0]
    for shift, radix in digits[:-1]:
        cur = [(d << shift) | m for d in range(radix) for m in cur]
    shift, radix = digits[-1]
    return [[(d << shift) | m for m in cur] for d in range(radix)]


def exchange(value, mask, swap=0):
    ep_count, tp_count = lax.axis_size("ep"), lax.axis_size("tp")
    pairs = [
        (e * tp_count + t, (e ^ mask) * tp_count + (t ^ swap)) for e in range(ep_count) for t in range(tp_count)
    ]
    return lax.ppermute(value, AXES, pairs)


def exchange_all(parts, shift, radix):
    got = [parts[0]]
    for d in range(1, radix):
        got.append(exchange(parts[d], d << shift))
    return got


def gather_xor(piece, digits):
    cur = piece[None]
    for shift, radix in digits[:-1]:
        cur = jnp.concatenate(exchange_all([cur] * radix, shift, radix), axis=0)
    shift, radix = digits[-1]
    return exchange_all([cur] * radix, shift, radix)


def scatter_masks(order):
    rest, done = [0], [0]
    for shift, radix in order[1:]:
        rest = [m | (d << shift) for m in rest for d in range(radix)]
    for shift, radix in order[:-1]:
        done = [(d << shift) | m for d in range(radix) for m in done]
    (first, first_radix), (last, last_radix) = order[0], order[-1]
    sent = [[(d << first) | m for m in rest] for d in range(first_radix)]
    return sent, [[(d << last) | m for m in done] for d in range(last_radix)]


def scatter_xor(parts, order):
    block = parts[0].shape[1:]
    for level, (shift, radix) in enumerate(order):
        got = exchange_all(parts, shift, radix)
        if level + 1 == len(order):
            return got
        nxt, rest = order[level + 1][1], 1
        for _, r in order[level + 2 :]:
            rest *= r
        got = [g.reshape(-1, nxt, rest, *block) for g in got]
        cut = jax.ShapeDtypeStruct((radix, got[0].shape[0], rest, *block), got[0].dtype)
        parts = call(cut_kernel, (cut,) * nxt, got, smem=())
        parts = [p.reshape(-1, *block) for p in parts]


def cut_kernel(*refs):
    radix = refs[-1].shape[0]
    for j, out in enumerate(refs[radix:]):
        for d in range(radix):
            out[d] = refs[d][:, j]


def scale_rows(values, gain):
    return values * lax.rsqrt(jnp.mean(values * values, axis=-1, keepdims=True) + EPS) * gain


def load_kernel(after, wq, wk, wv, wz, gain, state, stacked, gain_out, near, short, rows, sems, state_sems):
    each = wq.shape[0]
    copies = [
        pltpu.make_async_copy(ref, rows.at[pl.ds(p * each, each), :], sems.at[p]) for p, ref in enumerate((wq, wk, wv, wz))
    ]
    copies.append(pltpu.make_async_copy(gain, gain_out, sems.at[4]))
    for c in copies:
        c.start()
    seqs = state.shape[0]
    fetch = lambda i: pltpu.make_async_copy(state.at[i], near.at[i], state_sems.at[i])
    for i in range(seqs):
        fetch(i).start()
    for c in copies:
        c.wait()
    stacked[...] = rows[...].astype(F32).T.astype(BF16)

    def one(i, carry):
        fetch(i).wait()
        short[i] = near[i].astype(BF16)
        return carry

    lax.fori_loop(0, seqs, one, 0)


def norm_kernel(masks, where, *refs):
    pieces, gain, out = refs[: len(masks)], refs[-3], refs[-1]
    me = where[0]
    for ref, row in zip(pieces, masks):
        for j, mask in enumerate(row):
            out[me ^ mask] = scale_rows(ref[j].astype(F32), gain[...]).astype(BF16)


def project_own_kernel(x_ref, stacked, out):
    x = x_ref[...].reshape(-1, x_ref.shape[2])
    y = jnp.dot(x, stacked[...], preferred_element_type=F32)
    out[...] = y.reshape(out.shape).astype(BF16)


def project_kernel(sent, where, x_ref, own, stacked, *refs):
    outs, other = refs[:-1], refs[-1]
    me, par = where[0], where[1]
    project_own_kernel(x_ref, stacked, other)
    for out, row in zip(outs, sent):
        for j, mask in enumerate(row):
            out[j, par] = own[me ^ mask]
            out[j, 1 - par] = other[me ^ mask]


def rates_kernel(
    where, own, other, wb, wd, rate, bias, ids, chance, beta, retain, route, route_other, column
):
    me, par = where[0], where[1]
    for side, ref in ((par, own), (1 - par, other)):
        x = ref[me]
        b = lax.dot_general(x, wb[...], (((1,), (1,)), ((), ())), preferred_element_type=F32)
        d = lax.dot_general(x, wd[...], (((1,), (1,)), ((), ())), preferred_element_type=F32)
        d = d + bias[...]
        soft = jnp.maximum(d, 0.0) + jnp.log1p(jnp.exp(-jnp.abs(d)))
        beta[side] = 1.0 / (1.0 + jnp.exp(-b))
        retain[side] = jnp.exp(-rate[...] * soft)
    picked = jnp.sum(jnp.where(ids[...] == me, chance[...], 0.0), axis=0, keepdims=True)
    picked = jnp.broadcast_to(picked, (8, picked.shape[1])).T[:, :1]
    column[...] = picked.reshape(column.shape)
    route[...] = column[:, par].reshape(route.shape)
    route_other[...] = column[:, 1 - par].reshape(route.shape)


def silu(x):
    return x / (1.0 + jnp.exp(-x))


def regroup(blocks, piece):
    lane = lax.broadcasted_iota(jnp.int32, blocks[0].shape, 1) // piece
    step = 1
    while step < len(blocks):
        low = (lane & step) == 0
        blocks = list(blocks)
        for i in range(len(blocks)):
            if i & step:
                continue
            a, b = blocks[i], blocks[i | step]
            lanes = a.shape[1]
            blocks[i] = jnp.where(low, a, pltpu.roll(b, step * piece, 1))
            blocks[i | step] = jnp.where(low, pltpu.roll(a, lanes - step * piece, 1), b)
        step *= 2
    return blocks


def state_kernel(heads, came, where, *refs):
    pieces, (beta, retain, gain, near, short, gated, new_state) = refs[: len(came)], refs[len(came) : len(came) + 7]
    cols, rows, both, reads, lefts, new, sems = refs[len(came) + 7 :]
    for ref, row in zip(pieces, came):
        for j, mask in enumerate(row):
            cols[where[0] ^ mask] = ref[j].reshape(cols.shape[1:])
    seqs, size = near.shape[0], near.shape[2]
    store = lambda i: pltpu.make_async_copy(new.at[i], new_state.at[i], sems.at[i])
    count, width = cols.shape[0], cols.shape[2]
    piece = width // (4 * heads)
    for first in range(0, width, size):
        blocks = []
        for e in range(count):
            block = cols[e, :, first : min(first + size, width)].astype(F32)
            if block.shape[1] < size:
                block = jnp.concatenate([block, jnp.zeros((seqs, size - block.shape[1]), F32)], axis=1)
            blocks.append(block)
        for i, block in enumerate(regroup(blocks, piece)):
            n = first // piece + i
            if n < 4 * heads:
                rows[n // heads, pl.ds(n % heads, seqs, stride=heads), :] = block
    for h in range(heads):
        rows[4, pl.ds(h, seqs, stride=heads), :] = jnp.broadcast_to(beta[:, h : h + 1], (seqs, size))
        rows[5, pl.ds(h, seqs, stride=heads), :] = jnp.broadcast_to(retain[:, h : h + 1], (seqs, size))
    q = silu(rows[0])
    q = q * lax.rsqrt(jnp.sum(q * q, axis=-1, keepdims=True) + EPS) * size ** (-0.5)
    k = silu(rows[1])
    k = k * lax.rsqrt(jnp.sum(k * k, axis=-1, keepdims=True) + EPS)
    dots = jnp.sum(q * k, axis=-1, keepdims=True)
    owner = lax.broadcasted_iota(jnp.int32, (seqs, heads, size), 1)
    k3, q3 = k.reshape(seqs, heads, size), q.reshape(seqs, heads, size)
    for h in range(heads):
        at = slice(h * size, (h + 1) * size)
        both[:, :heads, at] = jnp.where(owner == h, k3, 0.0).astype(BF16)
        both[:, heads:, at] = jnp.where(owner == h, q3, 0.0).astype(BF16)
    for i in range(seqs):
        found = jnp.dot(both[i], short[i], preferred_element_type=F32)
        reads[0, i * heads : (i + 1) * heads, :] = found[:heads]
        reads[1, i * heads : (i + 1) * heads, :] = found[heads:]
    keep = rows[5]
    change = rows[4] * (silu(rows[2]) - keep * reads[0])
    reads[0] = change
    read = keep * reads[1] + dots * change
    reads[1] = scale_rows(read, gain[...]) * silu(rows[3])
    for h in range(heads):
        gated[:, h * size : (h + 1) * size] = reads[1, pl.ds(h, seqs, stride=heads), :].astype(BF16)
    high = k.astype(BF16).astype(F32)
    low = (k - high).astype(BF16).astype(F32)
    lefts[:, :heads] = high.reshape(seqs, heads, size)
    lefts[:, heads : 2 * heads] = high.reshape(seqs, heads, size)
    lefts[:, 2 * heads : 3 * heads] = low.reshape(seqs, heads, size)
    lefts[:, 3 * heads :] = jnp.zeros((seqs, lefts.shape[1] - 3 * heads, size), F32)
    head_row = lax.broadcasted_iota(jnp.int32, (lefts.shape[1], size), 0) % heads

    def one(i, carry):
        at = pl.ds(pl.multiple_of(i * heads, heads), heads)
        step = reads[0, at, :]
        top = step.astype(BF16).astype(F32)
        rest = step - top
        right = jnp.concatenate([top, rest, top, jnp.zeros_like(top)], axis=0)
        right = jnp.concatenate([jnp.where(head_row == h, right, 0.0).astype(BF16) for h in range(heads)], axis=1)
        added = jnp.dot(lefts[i].T.astype(BF16), right, preferred_element_type=F32)
        rate = rows[5, at, :]
        for h in range(heads):
            old = near[i, h * size : (h + 1) * size, :]
            new[i, h] = rate[h : h + 1, :] * old + added[:, h * size : (h + 1) * size]
        store(i).start()
        return carry

    lax.fori_loop(0, seqs, one, 0, unroll=2)
    for i in range(seqs):
        store(i).wait()


def run_state(came, where, pieces, beta, retain, gain, near, short, shape):
    seqs, heads, size = shape[:3]
    count, columns = sum(map(len, came)), pieces[0].shape[-1]
    sds = jax.ShapeDtypeStruct
    return call(
        functools.partial(state_kernel, heads, came),
        (sds((seqs, heads * size), BF16), sds(shape, F32)),
        [where, *pieces, beta, retain, gain, near, short],
        hbm_out=(1,),
        scratch=[
            VM((count, seqs, columns), BF16),
            VM((6, seqs * heads, size), F32),
            VM((seqs, 2 * heads, heads * size), BF16),
            VM((2, seqs * heads, size), F32),
            VM((seqs, 4 * heads, size), F32),
            VM(shape, F32),
            pltpu.SemaphoreType.DMA((seqs,)),
        ],
    )


def mix_kernel(masks, where, *refs):
    pieces, weight, out, out_other, both = refs[: len(masks)], *refs[-4:]
    me, par = where[0], where[1]
    each = out.shape[1]
    for ref, row in zip(pieces, masks):
        x = ref[...].reshape(-1, ref.shape[2])
        y = jnp.dot(x, weight[...], preferred_element_type=F32)
        y = y.reshape(len(row), 2, each, -1).astype(BF16)
        for j, mask in enumerate(row):
            for side in range(2):
                both[side, me ^ mask] = y[j, side]
    out[...] = both[par]
    out_other[...] = both[1 - par]


def pair_kernel(own, other, out):
    out[...] = (own[...].astype(F32) + other[...].astype(F32)).reshape(out.shape).astype(out.dtype)


def resid_kernel(masks, where, *refs):
    count = len(masks)
    tokens, mixed, gain = refs[:count], refs[count:-4], refs[-4]
    moe, own, resid = refs[-3:]
    me = where[0]
    each = own.shape[0]
    for ref, row in zip(tokens, masks):
        for j, mask in enumerate(row):
            at = pl.multiple_of((me ^ mask) * each, each)
            resid[pl.ds(at, each), :] = ref[j].astype(F32)
    if len(mixed) == 1:
        resid[...] = resid[...] + mixed[0][...].astype(F32)
    for ref, row in zip(mixed, masks if len(mixed) > 1 else ()):
        for j, mask in enumerate(row):
            width = ref.shape[2]
            at = pl.ds(pl.multiple_of((me ^ mask) * width, width), width)
            resid[:, at] = resid[:, at] + ref[j].astype(F32)
    moe[...] = scale_rows(resid[...], gain[...]).astype(BF16)
    own[...] = resid[pl.ds(pl.multiple_of(me * each, each), each), :]


def expert_kernel(rows_in, route, mix, d_gate, d_up, d_down, e_gate, e_up, e_down, out):
    x = rows_in[...]
    dot = functools.partial(jnp.dot, preferred_element_type=F32)
    hidden = (silu(dot(x, e_gate[...])) * dot(x, e_up[...])).astype(BF16)
    dense = (silu(dot(x, d_gate[...])) * dot(x, d_up[...])).astype(BF16)
    factor = jnp.sum(x.astype(F32) * mix[...].astype(F32), axis=1, keepdims=True)
    factor = 1.0 / (1.0 + jnp.exp(-factor))
    out[...] = (route[...] * dot(hidden, e_down[...]) + factor * dot(dense, d_down[...])).astype(out.dtype)


def fold_kernel(masks, where, own, other, *outs):
    me = where[0]
    each = outs[0].shape[1]
    for out, row in zip(outs, masks):
        for j, mask in enumerate(row):
            at = pl.ds(pl.multiple_of((me ^ mask) * each, each), each)
            out[j] = (own[at, :].astype(F32) + other[at, :].astype(F32)).astype(BF16)


def sum_kernel(parts, *refs):
    outs = refs[parts:]
    for i, out in enumerate(outs):
        total = refs[0][i].astype(F32)
        for ref in refs[1:parts]:
            total = total + ref[i].astype(F32)
        out[...] = total.astype(out.dtype)


def last_kernel(resid, *refs):
    total = refs[0][...].astype(F32)
    for ref in refs[1:-1]:
        total = total + ref[...].astype(F32)
    refs[-1][...] = (resid[...] + total).astype(refs[-1].dtype)


def body(
    tokens,
    mix_gain,
    w_query,
    w_key,
    w_value,
    w_zgate,
    w_beta,
    w_decay,
    decay_rate,
    decay_bias,
    head_gain,
    state,
    w_out,
    moe_gain,
    dense_mix,
    dense_gate,
    dense_up,
    dense_down,
    expert_gate,
    expert_up,
    expert_down,
    expert_ids,
    route_weight,
):
    ep_count = lax.axis_size("ep")
    me, par = lax.axis_index("ep"), lax.axis_index("tp")
    where = jnp.stack([me, par]).astype(jnp.int32)
    digits = digits_of(ep_count)
    masks = masks_of(digits)
    each, width = tokens.shape
    seqs, heads, size = state.shape[:3]
    half = ep_count * each
    sds = jax.ShapeDtypeStruct

    flat = [w.transpose(1, 2, 0).reshape(-1, width) for w in (w_query, w_key, w_value, w_zgate)]
    columns = 4 * flat[0].shape[0]
    tok_pieces = gather_xor(tokens, digits)
    stacked, gain_near, near, short = call(
        load_kernel,
        (
            sds((width, columns), BF16),
            sds((1, width), F32),
            sds((seqs, heads * size, size), F32),
            sds((seqs, heads * size, size), BF16),
        ),
        [tok_pieces[0], *flat, mix_gain[None], state.reshape(seqs, heads * size, size)],
        scratch=[VM((columns, width), BF16), pltpu.SemaphoreType.DMA((5,)), pltpu.SemaphoreType.DMA((seqs,))],
        smem=(),
        hbm=range(1, 7),
        loose=(0,),
        spare=6,
    )
    normed = call(
        functools.partial(norm_kernel, masks),
        sds((ep_count, each, width), BF16),
        [where, *tok_pieces, gain_near, stacked],
        loose=(len(masks) + 2,),
    )
    normed_other = exchange(normed, 0, 1)
    order = digits[::-1]
    sent, came = scatter_masks(order)
    projected = call(project_own_kernel, sds((ep_count, each, columns), BF16), [normed, stacked], smem=(), spare=3)
    projected = call(
        functools.partial(project_kernel, sent),
        tuple(sds((len(row), 2, each, columns), BF16) for row in sent),
        [where, normed_other, projected, stacked],
        scratch=[VM((ep_count, each, columns), BF16)],
        spare=3,
    )
    by_seq = scatter_xor(projected, order)
    beta, retain, route, route_other = call(
        rates_kernel,
        (
            sds((2, each, heads), F32),
            sds((2, each, heads), F32),
            sds((half, 1), F32),
            sds((half, 1), F32),
        ),
        [
            where,
            normed,
            normed_other,
            w_beta.T,
            w_decay.T,
            decay_rate[None],
            decay_bias[None],
            expert_ids.T,
            route_weight.T,
        ],
        scratch=[VM((ep_count, 2, each, 1), F32)],
    )
    gated, new_state = run_state(
        came,
        where,
        by_seq,
        beta.reshape(seqs, heads),
        retain.reshape(seqs, heads),
        head_gain[None],
        near,
        short,
        state.shape,
    )

    gated_pieces = gather_xor(gated, digits)
    out_cols = w_out.shape[1]
    mixed, mixed_other = call(
        functools.partial(mix_kernel, masks),
        (sds((ep_count, each, out_cols), BF16), sds((ep_count, each, out_cols), BF16)),
        [where, *gated_pieces, w_out],
        scratch=[VM((2, ep_count, each, out_cols), BF16)],
    )
    mixed_other = exchange(mixed_other, 0, 1)
    mixed = call(pair_kernel, sds((half, out_cols), BF16), [mixed, mixed_other], smem=())
    mixed_pieces = gather_xor(mixed, digits)
    if out_cols % 128:
        order = jnp.argsort(me ^ jnp.array([m for row in masks for m in row], jnp.int32))
        blocks = jnp.take(jnp.concatenate(mixed_pieces, axis=0), order, axis=0)
        mixed_pieces = [blocks.transpose(1, 0, 2).reshape(half, width)]
    moe_in, resid = call(
        functools.partial(resid_kernel, masks),
        (sds((half, width), BF16), sds((each, width), F32)),
        [where, *tok_pieces, *mixed_pieces, moe_gain[None]],
        scratch=[VM((half, width), F32)],
    )
    moe_other = exchange(moe_in, 0, 1)

    weights = [dense_mix[None], dense_gate, dense_up, dense_down, expert_gate[0], expert_up[0], expert_down[0]]
    run = lambda x, r, dt: call(expert_kernel, sds((half, width), dt), [x, r, *weights], smem=(), spare=6)
    part_own = run(moe_in, route, F32)
    part_other = run(moe_other, route_other, BF16)

    prev = len(masks[0])
    parts = call(
        functools.partial(fold_kernel, masks),
        tuple(sds((prev, each, width), BF16) for _ in masks),
        [where, part_own, exchange(part_other, 0, 1)],
    )
    for level in range(len(digits) - 1, 0, -1):
        shift, radix = digits[level]
        got = exchange_all(parts, shift, radix)
        nxt = digits[level - 1][1]
        got = [g.reshape(nxt, -1, width) for g in got]
        parts = call(
            functools.partial(sum_kernel, len(got)),
            tuple(sds(got[0].shape[1:], BF16) for _ in range(nxt)),
            got,
            smem=(),
        )
    shift, radix = digits[0]
    got = exchange_all(parts, shift, radix)
    layer_out = call(last_kernel, sds((each, width), BF16), [resid, *got], smem=())
    return (layer_out, new_state)


def solution(mesh):
    placed = (
        P(("ep", "tp"), None),
        P(),
        P(None, "tp", "ep"),
        P(None, "tp", "ep"),
        P(None, "tp", "ep"),
        P(None, "tp", "ep"),
        P(None, "tp"),
        P(None, "tp"),
        P("tp"),
        P("tp"),
        P(),
        P("ep", "tp", None, None),
        P("tp", "ep"),
        P(),
        P(),
        P(None, ("ep", "tp")),
        P(None, ("ep", "tp")),
        P(("ep", "tp"), None),
        P("ep", None, "tp"),
        P("ep", None, "tp"),
        P("ep", "tp", None),
        P(),
        P(),
    )
    return jax.shard_map(
        body,
        mesh=mesh,
        in_specs=placed,
        out_specs=(P(("ep", "tp"), None), P("ep", "tp", None, None)),
        check_vma=False,
    )
```

```python
import functools

import jax
import jax.numpy as jnp
from jax import lax
from jax.experimental import pallas as pl
from jax.experimental.pallas import tpu as pltpu
from jax.sharding import PartitionSpec as P


EPS = 1e-06
AXES = ("ep", "tp")
F32 = jnp.float32
BF16 = jnp.bfloat16
VM = pltpu.VMEM
SM = pltpu.SMEM


def padded_bytes(shape, dtype):
    shape = (1, 1) + tuple(shape)
    item = jnp.dtype(dtype).itemsize
    lead = 1
    for n in shape[:-2]:
        lead *= n
    return lead * -(-shape[-2] // 8) * 8 * -(-shape[-1] // 128) * 128 * item


def call(kernel, out_shape, operands, scratch=(), smem=(0,), hbm=(), loose=(), hbm_out=(), spare=2):
    outs, tree = jax.tree.flatten(out_shape)
    held = [x for i, x in enumerate(operands) if i not in smem and i not in hbm and i not in loose]
    held += [x for i, x in enumerate(outs) if i not in hbm_out]
    held += [x for x in scratch if hasattr(x, "shape") and getattr(x, "memory_space", None) == VM]
    limit = sum(padded_bytes(x.shape, x.dtype) for x in held) + (spare << 20)
    space = lambda i: SM if i in smem else pltpu.HBM if i in hbm else pl.ANY if i in loose else VM
    return pl.pallas_call(
        kernel,
        out_shape=out_shape,
        in_specs=[pl.BlockSpec(memory_space=space(i)) for i in range(len(operands))],
        out_specs=jax.tree.unflatten(
            tree, [pl.BlockSpec(memory_space=pltpu.HBM if i in hbm_out else VM) for i in range(len(outs))]
        ),
        scratch_shapes=list(scratch),
        compiler_params=pltpu.CompilerParams(vmem_limit_bytes=limit),
    )(*[pltpu.with_memory_space_constraint(x, pltpu.HBM) if i in hbm else x for i, x in enumerate(operands)])


def digits_of(count):
    bits = count.bit_length() - 1
    found = []
    while bits > 0:
        width = 2 if bits >= 2 else 1
        bits -= width
        found.append((bits, 1 << width))
    return found


def masks_of(digits):
    cur = [0]
    for shift, radix in digits[:-1]:
        cur = [(d << shift) | m for d in range(radix) for m in cur]
    shift, radix = digits[-1]
    return [[(d << shift) | m for m in cur] for d in range(radix)]


def exchange(value, mask, swap=0):
    ep_count, tp_count = lax.axis_size("ep"), lax.axis_size("tp")
    pairs = [
        (e * tp_count + t, (e ^ mask) * tp_count + (t ^ swap)) for e in range(ep_count) for t in range(tp_count)
    ]
    return lax.ppermute(value, AXES, pairs)


def exchange_all(parts, shift, radix):
    got = [parts[0]]
    for d in range(1, radix):
        got.append(exchange(parts[d], d << shift))
    return got


def gather_xor(piece, digits, near=None):
    cur = piece[None]
    for shift, radix in digits[:-1]:
        got = exchange_all([cur] * radix, shift, radix)
        if near is not None:
            got[0], near = near[None], None
        cur = jnp.concatenate(got, axis=0)
    shift, radix = digits[-1]
    return exchange_all([cur] * radix, shift, radix)


def scatter_masks(order):
    rest, done = [0], [0]
    for shift, radix in order[1:]:
        rest = [m | (d << shift) for m in rest for d in range(radix)]
    for shift, radix in order[:-1]:
        done = [(d << shift) | m for d in range(radix) for m in done]
    (first, first_radix), (last, last_radix) = order[0], order[-1]
    sent = [[(d << first) | m for m in rest] for d in range(first_radix)]
    return sent, [[(d << last) | m for m in done] for d in range(last_radix)]


def scatter_xor(parts, order):
    block = parts[0].shape[1:]
    for level, (shift, radix) in enumerate(order):
        got = exchange_all(parts, shift, radix)
        if level + 1 == len(order):
            return got
        nxt, rest = order[level + 1][1], 1
        for _, r in order[level + 2 :]:
            rest *= r
        got = [g.reshape(-1, nxt, rest, *block) for g in got]
        cut = jax.ShapeDtypeStruct((radix, got[0].shape[0], rest, *block), got[0].dtype)
        parts = call(cut_kernel, (cut,) * nxt, got, smem=())
        parts = [p.reshape(-1, *block) for p in parts]


def cut_kernel(*refs):
    radix = refs[-1].shape[0]
    for j, out in enumerate(refs[radix:]):
        for d in range(radix):
            out[d] = refs[d][:, j]


def scale_rows(values, gain):
    return values * lax.rsqrt(jnp.mean(values * values, axis=-1, keepdims=True) + EPS) * gain


def load_kernel(after, wq, wk, wv, wz, gain, state, stacked, gain_out, near, short, rows, sems, state_sems):
    each = wq.shape[0]
    copies = [
        pltpu.make_async_copy(ref, rows.at[pl.ds(p * each, each), :], sems.at[p]) for p, ref in enumerate((wq, wk, wv, wz))
    ]
    copies.append(pltpu.make_async_copy(gain, gain_out, sems.at[4]))
    for c in copies:
        c.start()
    seqs = state.shape[0]
    fetch = lambda i: pltpu.make_async_copy(state.at[i], near.at[i], state_sems.at[i])
    for i in range(seqs):
        fetch(i).start()
    for c in copies:
        c.wait()
    stacked[...] = rows[...].astype(F32).T.astype(BF16)

    def one(i, carry):
        fetch(i).wait()
        short[i] = near[i].astype(BF16)
        return carry

    lax.fori_loop(0, seqs, one, 0)


def norm_kernel(masks, where, *refs):
    pieces, gain, out = refs[: len(masks)], refs[-3], refs[-1]
    me = where[0]
    for ref, row in zip(pieces, masks):
        for j, mask in enumerate(row):
            out[me ^ mask] = scale_rows(ref[j].astype(F32), gain[...]).astype(BF16)


def project_own_kernel(x_ref, stacked, out):
    x = x_ref[...].reshape(-1, x_ref.shape[2])
    y = jnp.dot(x, stacked[...], preferred_element_type=F32)
    out[...] = y.reshape(out.shape).astype(BF16)


def project_kernel(sent, where, x_ref, own, stacked, *refs):
    outs, other = refs[:-1], refs[-1]
    me, par = where[0], where[1]
    project_own_kernel(x_ref, stacked, other)
    for out, row in zip(outs, sent):
        for j, mask in enumerate(row):
            out[j, par] = own[me ^ mask]
            out[j, 1 - par] = other[me ^ mask]


def rates_kernel(
    masks, where, own, other, wb, wd, rate, bias, ids, chance, *refs
):
    pieces, (beta, retain, route, route_other, ordered, column) = refs[: len(masks)], refs[len(masks) :]
    me, par = where[0], where[1]
    for ref, row in zip(pieces, masks):
        for j, mask in enumerate(row):
            ordered[me ^ mask] = ref[j]
    for side, ref in ((par, own), (1 - par, other)):
        x = ref[me]
        b = lax.dot_general(x, wb[...], (((1,), (1,)), ((), ())), preferred_element_type=F32)
        d = lax.dot_general(x, wd[...], (((1,), (1,)), ((), ())), preferred_element_type=F32)
        d = d + bias[...]
        soft = jnp.maximum(d, 0.0) + jnp.log1p(jnp.exp(-jnp.abs(d)))
        beta[side] = 1.0 / (1.0 + jnp.exp(-b))
        retain[side] = jnp.exp(-rate[...] * soft)
    picked = jnp.sum(jnp.where(ids[...] == me, chance[...], 0.0), axis=0, keepdims=True)
    picked = jnp.broadcast_to(picked, (8, picked.shape[1])).T[:, :1]
    column[...] = picked.reshape(column.shape)
    route[...] = column[:, par].reshape(route.shape)
    route_other[...] = column[:, 1 - par].reshape(route.shape)


def silu(x):
    return x / (1.0 + jnp.exp(-x))


def regroup(blocks, piece):
    lane = lax.broadcasted_iota(jnp.int32, blocks[0].shape, 1) // piece
    step = 1
    while step < len(blocks):
        low = (lane & step) == 0
        blocks = list(blocks)
        for i in range(len(blocks)):
            if i & step:
                continue
            a, b = blocks[i], blocks[i | step]
            lanes = a.shape[1]
            blocks[i] = jnp.where(low, a, pltpu.roll(b, step * piece, 1))
            blocks[i | step] = jnp.where(low, pltpu.roll(a, lanes - step * piece, 1), b)
        step *= 2
    return blocks


def state_kernel(heads, came, where, *refs):
    pieces, (beta, retain, gain, short, gated, k_out, keep_out, change_out) = (
        refs[: len(came)],
        refs[len(came) : len(came) + 8],
    )
    cols, rows, both, reads = refs[len(came) + 8 :]
    for ref, row in zip(pieces, came):
        for j, mask in enumerate(row):
            cols[where[0] ^ mask] = ref[j].reshape(cols.shape[1:])
    seqs, size = short.shape[0], short.shape[2]
    count, width = cols.shape[0], cols.shape[2]
    piece = width // (4 * heads)
    for first in range(0, width, size):
        blocks = []
        for e in range(count):
            block = cols[e, :, first : min(first + size, width)].astype(F32)
            if block.shape[1] < size:
                block = jnp.concatenate([block, jnp.zeros((seqs, size - block.shape[1]), F32)], axis=1)
            blocks.append(block)
        for i, block in enumerate(regroup(blocks, piece)):
            n = first // piece + i
            if n < 4 * heads:
                rows[n // heads, pl.ds(n % heads, seqs, stride=heads), :] = block
    for h in range(heads):
        rows[4, pl.ds(h, seqs, stride=heads), :] = jnp.broadcast_to(beta[:, h : h + 1], (seqs, size))
        rows[5, pl.ds(h, seqs, stride=heads), :] = jnp.broadcast_to(retain[:, h : h + 1], (seqs, size))
    q = silu(rows[0])
    q = q * lax.rsqrt(jnp.sum(q * q, axis=-1, keepdims=True) + EPS) * size ** (-0.5)
    k = silu(rows[1])
    k = k * lax.rsqrt(jnp.sum(k * k, axis=-1, keepdims=True) + EPS)
    dots = jnp.sum(q * k, axis=-1, keepdims=True)
    owner = lax.broadcasted_iota(jnp.int32, (seqs, heads, size), 1)
    k3, q3 = k.reshape(seqs, heads, size), q.reshape(seqs, heads, size)
    for h in range(heads):
        at = slice(h * size, (h + 1) * size)
        both[:, :heads, at] = jnp.where(owner == h, k3, 0.0).astype(BF16)
        both[:, heads:, at] = jnp.where(owner == h, q3, 0.0).astype(BF16)
    for i in range(seqs):
        found = jnp.dot(both[i], short[i], preferred_element_type=F32)
        reads[0, i * heads : (i + 1) * heads, :] = found[:heads]
        reads[1, i * heads : (i + 1) * heads, :] = found[heads:]
    keep = rows[5]
    change = rows[4] * (silu(rows[2]) - keep * reads[0])
    k_out[...], keep_out[...], change_out[...] = k, keep, change
    read = keep * reads[1] + dots * change
    reads[1] = scale_rows(read, gain[...]) * silu(rows[3])
    for h in range(heads):
        gated[:, h * size : (h + 1) * size] = reads[1, pl.ds(h, seqs, stride=heads), :].astype(BF16)


def store_kernel(heads, k_in, keep, change, near, after, new_state, lefts, new, sems):
    seqs, size = near.shape[0], near.shape[2]
    store = lambda i: pltpu.make_async_copy(new.at[i], new_state.at[i], sems.at[i])
    k = k_in[...]
    high = k.astype(BF16).astype(F32)
    low = (k - high).astype(BF16).astype(F32)
    lefts[:, :heads] = high.reshape(seqs, heads, size)
    lefts[:, heads : 2 * heads] = high.reshape(seqs, heads, size)
    lefts[:, 2 * heads : 3 * heads] = low.reshape(seqs, heads, size)
    lefts[:, 3 * heads :] = jnp.zeros((seqs, lefts.shape[1] - 3 * heads, size), F32)
    head_row = lax.broadcasted_iota(jnp.int32, (lefts.shape[1], size), 0) % heads

    def one(i, carry):
        at = pl.ds(pl.multiple_of(i * heads, heads), heads)
        step = change[at, :]
        top = step.astype(BF16).astype(F32)
        rest = step - top
        right = jnp.concatenate([top, rest, top, jnp.zeros_like(top)], axis=0)
        right = jnp.concatenate([jnp.where(head_row == h, right, 0.0).astype(BF16) for h in range(heads)], axis=1)
        added = jnp.dot(lefts[i].T.astype(BF16), right, preferred_element_type=F32)
        rate = keep[at, :]
        for h in range(heads):
            old = near[i, h * size : (h + 1) * size, :]
            new[i, h] = rate[h : h + 1, :] * old + added[:, h * size : (h + 1) * size]
        store(i).start()
        return carry

    lax.fori_loop(0, seqs, one, 0, unroll=2)
    for i in range(seqs):
        store(i).wait()


def run_state(came, where, pieces, beta, retain, gain, short, shape):
    seqs, heads, size = shape[:3]
    count, columns = sum(map(len, came)), pieces[0].shape[-1]
    sds = jax.ShapeDtypeStruct
    per_head = sds((seqs * heads, size), F32)
    return call(
        functools.partial(state_kernel, heads, came),
        (sds((seqs, heads * size), BF16), per_head, per_head, per_head),
        [where, *pieces, beta, retain, gain, short],
        scratch=[
            VM((count, seqs, columns), BF16),
            VM((6, seqs * heads, size), F32),
            VM((seqs, 2 * heads, heads * size), BF16),
            VM((2, seqs * heads, size), F32),
        ],
    )


def run_store(k, keep, change, near, after, shape):
    seqs, heads, size = shape[:3]
    return call(
        functools.partial(store_kernel, heads),
        jax.ShapeDtypeStruct(shape, F32),
        [k, keep, change, near, after],
        smem=(),
        loose=(4,),
        hbm_out=(0,),
        scratch=[VM((seqs, 4 * heads, size), F32), VM(shape, F32), pltpu.SemaphoreType.DMA((seqs,))],
    )


def copy_kernel(source, out):
    out[...] = source[...]


def mix_kernel(masks, where, *refs):
    pieces, weight, out, out_other, both = refs[: len(masks)], *refs[-4:]
    me, par = where[0], where[1]
    each = out.shape[1]
    for ref, row in zip(pieces, masks):
        x = ref[...].reshape(-1, ref.shape[2])
        y = jnp.dot(x, weight[...], preferred_element_type=F32)
        y = y.reshape(len(row), 2, each, -1).astype(BF16)
        for j, mask in enumerate(row):
            for side in range(2):
                both[side, me ^ mask] = y[j, side]
    out[...] = both[par]
    out_other[...] = both[1 - par]


def pair_kernel(own, other, out):
    out[...] = (own[...].astype(F32) + other[...].astype(F32)).reshape(out.shape).astype(out.dtype)


def resid_kernel(masks, where, tokens, *refs):
    mixed, (gain, moe, own, resid) = refs[:-4], refs[-4:]
    me = where[0]
    count, each, size = tokens.shape
    squares = None
    for ref, row in zip(mixed, masks):
        for j, mask in enumerate(row):
            wide = ref.shape[2]
            at = pl.ds(pl.multiple_of((me ^ mask) * wide, wide), wide) if len(row) * len(mixed) > 1 else slice(None)
            part = tokens[:, :, at].astype(F32).reshape(count * each, wide) + ref[j].astype(F32)
            resid[:, at] = part
            squares = part * part if squares is None else squares + part * part
    scale = lax.rsqrt(jnp.sum(squares, axis=-1, keepdims=True) / size + EPS)
    moe[...] = (resid[...] * scale * gain[...]).astype(BF16)
    own[...] = resid[pl.ds(pl.multiple_of(me * each, each), each), :]


def expert_kernel(rows_in, route, mix, d_gate, d_up, d_down, e_gate, e_up, e_down, out):
    x = rows_in[...]
    dot = functools.partial(jnp.dot, preferred_element_type=F32)
    hidden = (silu(dot(x, e_gate[...])) * dot(x, e_up[...])).astype(BF16)
    dense = (silu(dot(x, d_gate[...])) * dot(x, d_up[...])).astype(BF16)
    factor = jnp.sum(x.astype(F32) * mix[...].astype(F32), axis=1, keepdims=True)
    factor = 1.0 / (1.0 + jnp.exp(-factor))
    out[...] = (route[...] * dot(hidden, e_down[...]) + factor * dot(dense, d_down[...])).astype(out.dtype)


def fold_kernel(masks, where, own, other, *outs):
    me = where[0]
    each = outs[0].shape[1]
    for out, row in zip(outs, masks):
        for j, mask in enumerate(row):
            at = pl.ds(pl.multiple_of((me ^ mask) * each, each), each)
            out[j] = (own[at, :].astype(F32) + other[at, :].astype(F32)).astype(BF16)


def sum_kernel(parts, *refs):
    outs = refs[parts:]
    for i, out in enumerate(outs):
        total = refs[0][i].astype(F32)
        for ref in refs[1:parts]:
            total = total + ref[i].astype(F32)
        out[...] = total.astype(out.dtype)


def last_kernel(resid, *refs):
    total = refs[0][...].astype(F32)
    for ref in refs[1:-1]:
        total = total + ref[...].astype(F32)
    refs[-1][...] = (resid[...] + total).astype(refs[-1].dtype)


def body(
    tokens,
    mix_gain,
    w_query,
    w_key,
    w_value,
    w_zgate,
    w_beta,
    w_decay,
    decay_rate,
    decay_bias,
    head_gain,
    state,
    w_out,
    moe_gain,
    dense_mix,
    dense_gate,
    dense_up,
    dense_down,
    expert_gate,
    expert_up,
    expert_down,
    expert_ids,
    route_weight,
):
    ep_count = lax.axis_size("ep")
    me, par = lax.axis_index("ep"), lax.axis_index("tp")
    where = jnp.stack([me, par]).astype(jnp.int32)
    digits = digits_of(ep_count)
    masks = masks_of(digits)
    each, width = tokens.shape
    seqs, heads, size = state.shape[:3]
    half = ep_count * each
    sds = jax.ShapeDtypeStruct

    flat = [w.transpose(1, 2, 0).reshape(-1, width) for w in (w_query, w_key, w_value, w_zgate)]
    columns = 4 * flat[0].shape[0]
    near_tokens = call(copy_kernel, sds(tokens.shape, BF16), [tokens], smem=())
    tok_pieces = gather_xor(tokens, digits, near_tokens)
    stacked, gain_near, near, short = call(
        load_kernel,
        (
            sds((width, columns), BF16),
            sds((1, width), F32),
            sds((seqs, heads * size, size), F32),
            sds((seqs, heads * size, size), BF16),
        ),
        [tok_pieces[0], *flat, mix_gain[None], state.reshape(seqs, heads * size, size)],
        scratch=[VM((columns, width), BF16), pltpu.SemaphoreType.DMA((5,)), pltpu.SemaphoreType.DMA((seqs,))],
        smem=(),
        hbm=range(1, 7),
        loose=(0,),
        spare=6,
    )
    normed = call(
        functools.partial(norm_kernel, masks),
        sds((ep_count, each, width), BF16),
        [where, *tok_pieces, gain_near, stacked],
        loose=(len(masks) + 2,),
    )
    normed_other = exchange(normed, 0, 1)
    order = digits[::-1]
    sent, came = scatter_masks(order)
    projected = call(project_own_kernel, sds((ep_count, each, columns), BF16), [normed, stacked], smem=(), spare=3)
    projected = call(
        functools.partial(project_kernel, sent),
        tuple(sds((len(row), 2, each, columns), BF16) for row in sent),
        [where, normed_other, projected, stacked],
        scratch=[VM((ep_count, each, columns), BF16)],
        spare=3,
    )
    by_seq = scatter_xor(projected, order)
    beta, retain, route, route_other, ordered = call(
        functools.partial(rates_kernel, masks),
        (
            sds((2, each, heads), F32),
            sds((2, each, heads), F32),
            sds((half, 1), F32),
            sds((half, 1), F32),
            sds((ep_count, each, width), BF16),
        ),
        [
            where,
            normed,
            normed_other,
            w_beta.T,
            w_decay.T,
            decay_rate[None],
            decay_bias[None],
            expert_ids.T,
            route_weight.T,
            *tok_pieces,
        ],
        scratch=[VM((ep_count, 2, each, 1), F32)],
    )
    gated, k_rows, keep, change = run_state(
        came,
        where,
        by_seq,
        beta.reshape(seqs, heads),
        retain.reshape(seqs, heads),
        head_gain[None],
        short,
        state.shape,
    )

    gated_pieces = gather_xor(gated, digits)
    new_state = run_store(k_rows, keep, change, near, gated_pieces[0], state.shape)
    out_cols = w_out.shape[1]
    mixed, mixed_other = call(
        functools.partial(mix_kernel, masks),
        (sds((ep_count, each, out_cols), BF16), sds((ep_count, each, out_cols), BF16)),
        [where, *gated_pieces, w_out],
        scratch=[VM((2, ep_count, each, out_cols), BF16)],
    )
    mixed_other = exchange(mixed_other, 0, 1)
    mixed = call(pair_kernel, sds((half, out_cols), BF16), [mixed, mixed_other], smem=())
    mixed_pieces = gather_xor(mixed, digits)
    if out_cols % 128:
        order = jnp.argsort(me ^ jnp.array([m for row in masks for m in row], jnp.int32))
        blocks = jnp.take(jnp.concatenate(mixed_pieces, axis=0), order, axis=0)
        mixed_pieces = [blocks.transpose(1, 0, 2).reshape(1, half, width)]
    moe_in, resid = call(
        functools.partial(resid_kernel, masks if out_cols % 128 == 0 else [[0]]),
        (sds((half, width), BF16), sds((each, width), F32)),
        [where, ordered, *mixed_pieces, moe_gain[None]],
        scratch=[VM((half, width), F32)],
    )
    moe_other = exchange(moe_in, 0, 1)

    weights = [dense_mix[None], dense_gate, dense_up, dense_down, expert_gate[0], expert_up[0], expert_down[0]]
    run = lambda x, r, dt: call(expert_kernel, sds((half, width), dt), [x, r, *weights], smem=(), spare=6)
    part_own = run(moe_in, route, F32)
    part_other = run(moe_other, route_other, BF16)

    prev = len(masks[0])
    parts = call(
        functools.partial(fold_kernel, masks),
        tuple(sds((prev, each, width), BF16) for _ in masks),
        [where, part_own, exchange(part_other, 0, 1)],
    )
    for level in range(len(digits) - 1, 0, -1):
        shift, radix = digits[level]
        got = exchange_all(parts, shift, radix)
        nxt = digits[level - 1][1]
        got = [g.reshape(nxt, -1, width) for g in got]
        parts = call(
            functools.partial(sum_kernel, len(got)),
            tuple(sds(got[0].shape[1:], BF16) for _ in range(nxt)),
            got,
            smem=(),
        )
    shift, radix = digits[0]
    got = exchange_all(parts, shift, radix)
    layer_out = call(last_kernel, sds((each, width), BF16), [resid, *got], smem=())
    return (layer_out, new_state)


def solution(mesh):
    placed = (
        P(("ep", "tp"), None),
        P(),
        P(None, "tp", "ep"),
        P(None, "tp", "ep"),
        P(None, "tp", "ep"),
        P(None, "tp", "ep"),
        P(None, "tp"),
        P(None, "tp"),
        P("tp"),
        P("tp"),
        P(),
        P("ep", "tp", None, None),
        P("tp", "ep"),
        P(),
        P(),
        P(None, ("ep", "tp")),
        P(None, ("ep", "tp")),
        P(("ep", "tp"), None),
        P("ep", None, "tp"),
        P("ep", None, "tp"),
        P("ep", "tp", None),
        P(),
        P(),
    )
    return jax.shard_map(
        body,
        mesh=mesh,
        in_specs=placed,
        out_specs=(P(("ep", "tp"), None), P("ep", "tp", None, None)),
        check_vma=False,
    )
```

```python
import functools

import jax
import jax.numpy as jnp
from jax import lax
from jax.experimental import pallas as pl
from jax.experimental.pallas import tpu as pltpu
from jax.sharding import PartitionSpec as P


EPS = 1e-06
AXES = ("ep", "tp")
F32 = jnp.float32
BF16 = jnp.bfloat16
VM = pltpu.VMEM
SM = pltpu.SMEM


def padded_bytes(shape, dtype):
    shape = (1, 1) + tuple(shape)
    item = jnp.dtype(dtype).itemsize
    lead = 1
    for n in shape[:-2]:
        lead *= n
    return lead * -(-shape[-2] // 8) * 8 * -(-shape[-1] // 128) * 128 * item


def call(kernel, out_shape, operands, scratch=(), smem=(0,), hbm=(), loose=(), hbm_out=(), spare=2):
    outs, tree = jax.tree.flatten(out_shape)
    held = [x for i, x in enumerate(operands) if i not in smem and i not in hbm and i not in loose]
    held += [x for i, x in enumerate(outs) if i not in hbm_out]
    held += [x for x in scratch if hasattr(x, "shape") and getattr(x, "memory_space", None) == VM]
    limit = sum(padded_bytes(x.shape, x.dtype) for x in held) + (spare << 20)
    space = lambda i: SM if i in smem else pltpu.HBM if i in hbm else pl.ANY if i in loose else VM
    return pl.pallas_call(
        kernel,
        out_shape=out_shape,
        in_specs=[pl.BlockSpec(memory_space=space(i)) for i in range(len(operands))],
        out_specs=jax.tree.unflatten(
            tree, [pl.BlockSpec(memory_space=pltpu.HBM if i in hbm_out else VM) for i in range(len(outs))]
        ),
        scratch_shapes=list(scratch),
        compiler_params=pltpu.CompilerParams(vmem_limit_bytes=limit),
    )(*[pltpu.with_memory_space_constraint(x, pltpu.HBM) if i in hbm else x for i, x in enumerate(operands)])


def digits_of(count):
    bits = count.bit_length() - 1
    found = []
    while bits > 0:
        width = 2 if bits >= 2 else 1
        bits -= width
        found.append((bits, 1 << width))
    return found


def masks_of(digits):
    cur = [0]
    for shift, radix in digits[:-1]:
        cur = [(d << shift) | m for d in range(radix) for m in cur]
    shift, radix = digits[-1]
    return [[(d << shift) | m for m in cur] for d in range(radix)]


def exchange(value, mask, swap=0):
    ep_count, tp_count = lax.axis_size("ep"), lax.axis_size("tp")
    pairs = [
        (e * tp_count + t, (e ^ mask) * tp_count + (t ^ swap)) for e in range(ep_count) for t in range(tp_count)
    ]
    return lax.ppermute(value, AXES, pairs)


def exchange_all(parts, shift, radix):
    got = [parts[0]]
    for d in range(1, radix):
        got.append(exchange(parts[d], d << shift))
    return got


def gather_xor(piece, digits, near=None):
    cur = piece[None]
    for shift, radix in digits[:-1]:
        got = exchange_all([cur] * radix, shift, radix)
        if near is not None:
            got[0], near = near[None], None
        cur = jnp.concatenate(got, axis=0)
    shift, radix = digits[-1]
    return exchange_all([cur] * radix, shift, radix)


def scatter_masks(order):
    rest, done = [0], [0]
    for shift, radix in order[1:]:
        rest = [m | (d << shift) for m in rest for d in range(radix)]
    for shift, radix in order[:-1]:
        done = [(d << shift) | m for d in range(radix) for m in done]
    (first, first_radix), (last, last_radix) = order[0], order[-1]
    sent = [[(d << first) | m for m in rest] for d in range(first_radix)]
    return sent, [[(d << last) | m for m in done] for d in range(last_radix)]


def scatter_xor(parts, order):
    block = parts[0].shape[1:]
    for level, (shift, radix) in enumerate(order):
        got = exchange_all(parts, shift, radix)
        if level + 1 == len(order):
            return got
        nxt, rest = order[level + 1][1], 1
        for _, r in order[level + 2 :]:
            rest *= r
        got = [g.reshape(-1, nxt, rest, *block) for g in got]
        cut = jax.ShapeDtypeStruct((radix, got[0].shape[0], rest, *block), got[0].dtype)
        parts = call(cut_kernel, (cut,) * nxt, got, smem=())
        parts = [p.reshape(-1, *block) for p in parts]


def cut_kernel(*refs):
    radix = refs[-1].shape[0]
    for j, out in enumerate(refs[radix:]):
        for d in range(radix):
            out[d] = refs[d][:, j]


def scale_rows(values, gain):
    return values * lax.rsqrt(jnp.mean(values * values, axis=-1, keepdims=True) + EPS) * gain


def load_kernel(after, wq, wk, wv, wz, gain, state, stacked, gain_out, near, short, rows, sems, state_sems):
    each = wq.shape[0]
    copies = [
        pltpu.make_async_copy(ref, rows.at[pl.ds(p * each, each), :], sems.at[p]) for p, ref in enumerate((wq, wk, wv, wz))
    ]
    copies.append(pltpu.make_async_copy(gain, gain_out, sems.at[4]))
    for c in copies:
        c.start()
    first = state.shape[0] - near.shape[0]
    begin_state(first, state, near, state_sems)
    for c in copies:
        c.wait()
    stacked[...] = rows[...].astype(F32).T.astype(BF16)
    finish_state(first, state, near, short, state_sems)


def begin_state(first, state, near, sems):
    for i in range(near.shape[0]):
        pltpu.make_async_copy(state.at[first + i], near.at[i], sems.at[i]).start()


def finish_state(first, state, near, short, sems):
    def one(i, carry):
        pltpu.make_async_copy(state.at[first + i], near.at[i], sems.at[i]).wait()
        short[i] = near[i].astype(BF16)
        return carry

    lax.fori_loop(0, near.shape[0], one, 0)


def bring_kernel(after, tokens, state, tokens_out, near, short, sem, sems):
    copy = pltpu.make_async_copy(tokens, tokens_out, sem)
    copy.start()
    begin_state(0, state, near, sems)
    copy.wait()
    finish_state(0, state, near, short, sems)


def norm_kernel(masks, where, *refs):
    pieces, gain, out = refs[: len(masks)], refs[-3], refs[-1]
    me = where[0]
    for ref, row in zip(pieces, masks):
        for j, mask in enumerate(row):
            out[me ^ mask] = scale_rows(ref[j].astype(F32), gain[...]).astype(BF16)


def project_own_kernel(x_ref, stacked, out):
    x = x_ref[...].reshape(-1, x_ref.shape[2])
    y = jnp.dot(x, stacked[...], preferred_element_type=F32)
    out[...] = y.reshape(out.shape).astype(BF16)


def project_kernel(sent, where, x_ref, own, stacked, *refs):
    outs, other = refs[:-1], refs[-1]
    me, par = where[0], where[1]
    project_own_kernel(x_ref, stacked, other)
    for out, row in zip(outs, sent):
        for j, mask in enumerate(row):
            out[j, par] = own[me ^ mask]
            out[j, 1 - par] = other[me ^ mask]


def rates_kernel(
    masks, where, own, other, wb, wd, rate, bias, ids, chance, *refs
):
    pieces, (beta, retain, route, route_other, ordered, column) = refs[: len(masks)], refs[len(masks) :]
    me, par = where[0], where[1]
    for ref, row in zip(pieces, masks):
        for j, mask in enumerate(row):
            ordered[me ^ mask] = ref[j]
    for side, ref in ((par, own), (1 - par, other)):
        x = ref[me]
        b = lax.dot_general(x, wb[...], (((1,), (1,)), ((), ())), preferred_element_type=F32)
        d = lax.dot_general(x, wd[...], (((1,), (1,)), ((), ())), preferred_element_type=F32)
        d = d + bias[...]
        soft = jnp.maximum(d, 0.0) + jnp.log1p(jnp.exp(-jnp.abs(d)))
        beta[side] = 1.0 / (1.0 + jnp.exp(-b))
        retain[side] = jnp.exp(-rate[...] * soft)
    picked = jnp.sum(jnp.where(ids[...] == me, chance[...], 0.0), axis=0, keepdims=True)
    picked = jnp.broadcast_to(picked, (8, picked.shape[1])).T[:, :1]
    column[...] = picked.reshape(column.shape)
    route[...] = column[:, par].reshape(route.shape)
    route_other[...] = column[:, 1 - par].reshape(route.shape)


def silu(x):
    return x / (1.0 + jnp.exp(-x))


def regroup(blocks, piece):
    lane = lax.broadcasted_iota(jnp.int32, blocks[0].shape, 1) // piece
    step = 1
    while step < len(blocks):
        low = (lane & step) == 0
        blocks = list(blocks)
        for i in range(len(blocks)):
            if i & step:
                continue
            a, b = blocks[i], blocks[i | step]
            lanes = a.shape[1]
            blocks[i] = jnp.where(low, a, pltpu.roll(b, step * piece, 1))
            blocks[i | step] = jnp.where(low, pltpu.roll(a, lanes - step * piece, 1), b)
        step *= 2
    return blocks


def state_kernel(heads, came, where, *refs):
    pieces, (beta, retain, gain, *shorts, gated, k_out, keep_out, change_out) = (
        refs[: len(came)],
        refs[len(came) : -4],
    )
    cols, rows, both, reads = refs[-4:]
    for ref, row in zip(pieces, came):
        for j, mask in enumerate(row):
            cols[where[0] ^ mask] = ref[j].reshape(cols.shape[1:])
    seqs, size = cols.shape[1], shorts[0].shape[2]
    count, width = cols.shape[0], cols.shape[2]
    piece = width // (4 * heads)
    for first in range(0, width, size):
        blocks = []
        for e in range(count):
            block = cols[e, :, first : min(first + size, width)].astype(F32)
            if block.shape[1] < size:
                block = jnp.concatenate([block, jnp.zeros((seqs, size - block.shape[1]), F32)], axis=1)
            blocks.append(block)
        for i, block in enumerate(regroup(blocks, piece)):
            n = first // piece + i
            if n < 4 * heads:
                rows[n // heads, pl.ds(n % heads, seqs, stride=heads), :] = block
    for h in range(heads):
        rows[4, pl.ds(h, seqs, stride=heads), :] = jnp.broadcast_to(beta[:, h : h + 1], (seqs, size))
        rows[5, pl.ds(h, seqs, stride=heads), :] = jnp.broadcast_to(retain[:, h : h + 1], (seqs, size))
    q = silu(rows[0])
    q = q * lax.rsqrt(jnp.sum(q * q, axis=-1, keepdims=True) + EPS) * size ** (-0.5)
    k = silu(rows[1])
    k = k * lax.rsqrt(jnp.sum(k * k, axis=-1, keepdims=True) + EPS)
    dots = jnp.sum(q * k, axis=-1, keepdims=True)
    owner = lax.broadcasted_iota(jnp.int32, (seqs, heads, size), 1)
    k3, q3 = k.reshape(seqs, heads, size), q.reshape(seqs, heads, size)
    for h in range(heads):
        at = slice(h * size, (h + 1) * size)
        both[:, :heads, at] = jnp.where(owner == h, k3, 0.0).astype(BF16)
        both[:, heads:, at] = jnp.where(owner == h, q3, 0.0).astype(BF16)
    places = [(short, i) for short in shorts for i in range(short.shape[0])]
    for i, (short, j) in enumerate(places):
        found = jnp.dot(both[i], short[j], preferred_element_type=F32)
        reads[0, i * heads : (i + 1) * heads, :] = found[:heads]
        reads[1, i * heads : (i + 1) * heads, :] = found[heads:]
    keep = rows[5]
    change = rows[4] * (silu(rows[2]) - keep * reads[0])
    k_out[...], keep_out[...], change_out[...] = k, keep, change
    read = keep * reads[1] + dots * change
    reads[1] = scale_rows(read, gain[...]) * silu(rows[3])
    for h in range(heads):
        gated[:, h * size : (h + 1) * size] = reads[1, pl.ds(h, seqs, stride=heads), :].astype(BF16)


def store_kernel(heads, k_in, keep, change, near, near_late, after, new_state, lefts, new, sems):
    seqs, size = new.shape[0], near.shape[2]
    store = lambda i: pltpu.make_async_copy(new.at[i], new_state.at[i], sems.at[i])
    k = k_in[...]
    high = k.astype(BF16).astype(F32)
    low = (k - high).astype(BF16).astype(F32)
    lefts[:, :heads] = high.reshape(seqs, heads, size)
    lefts[:, heads : 2 * heads] = high.reshape(seqs, heads, size)
    lefts[:, 2 * heads : 3 * heads] = low.reshape(seqs, heads, size)
    lefts[:, 3 * heads :] = jnp.zeros((seqs, lefts.shape[1] - 3 * heads, size), F32)
    head_row = lax.broadcasted_iota(jnp.int32, (lefts.shape[1], size), 0) % heads

    def one(source, first, n, carry):
        i = first + n
        at = pl.ds(pl.multiple_of(i * heads, heads), heads)
        step = change[at, :]
        top = step.astype(BF16).astype(F32)
        rest = step - top
        right = jnp.concatenate([top, rest, top, jnp.zeros_like(top)], axis=0)
        right = jnp.concatenate([jnp.where(head_row == h, right, 0.0).astype(BF16) for h in range(heads)], axis=1)
        added = jnp.dot(lefts[i].T.astype(BF16), right, preferred_element_type=F32)
        rate = keep[at, :]
        for h in range(heads):
            old = source[n, h * size : (h + 1) * size, :]
            new[i, h] = rate[h : h + 1, :] * old + added[:, h * size : (h + 1) * size]
        store(i).start()
        return carry

    early = near.shape[0]
    lax.fori_loop(0, early, functools.partial(one, near, 0), 0, unroll=2)
    lax.fori_loop(0, seqs - early, functools.partial(one, near_late, early), 0, unroll=2)
    for i in range(seqs):
        store(i).wait()


def run_state(came, where, pieces, beta, retain, gain, shorts, shape):
    seqs, heads, size = shape[:3]
    count, columns = sum(map(len, came)), pieces[0].shape[-1]
    sds = jax.ShapeDtypeStruct
    per_head = sds((seqs * heads, size), F32)
    return call(
        functools.partial(state_kernel, heads, came),
        (sds((seqs, heads * size), BF16), per_head, per_head, per_head),
        [where, *pieces, beta, retain, gain, *shorts],
        scratch=[
            VM((count, seqs, columns), BF16),
            VM((6, seqs * heads, size), F32),
            VM((seqs, 2 * heads, heads * size), BF16),
            VM((2, seqs * heads, size), F32),
        ],
    )


def run_store(k, keep, change, near, near_late, after, shape):
    seqs, heads, size = shape[:3]
    return call(
        functools.partial(store_kernel, heads),
        jax.ShapeDtypeStruct(shape, F32),
        [k, keep, change, near, near_late, after],
        smem=(),
        loose=(5,),
        hbm_out=(0,),
        scratch=[VM((seqs, 4 * heads, size), F32), VM(shape, F32), pltpu.SemaphoreType.DMA((seqs,))],
    )


def mix_kernel(masks, where, *refs):
    pieces, weight, out, out_other, both = refs[: len(masks)], *refs[-4:]
    me, par = where[0], where[1]
    each = out.shape[1]
    for ref, row in zip(pieces, masks):
        x = ref[...].reshape(-1, ref.shape[2])
        y = jnp.dot(x, weight[...], preferred_element_type=F32)
        y = y.reshape(len(row), 2, each, -1).astype(BF16)
        for j, mask in enumerate(row):
            for side in range(2):
                both[side, me ^ mask] = y[j, side]
    out[...] = both[par]
    out_other[...] = both[1 - par]


def pair_kernel(own, other, out):
    out[...] = (own[...].astype(F32) + other[...].astype(F32)).reshape(out.shape).astype(out.dtype)


def resid_kernel(masks, where, tokens, *refs):
    mixed, (gain, moe, own, resid) = refs[:-4], refs[-4:]
    me = where[0]
    count, each, size = tokens.shape
    squares = None
    for ref, row in zip(mixed, masks):
        for j, mask in enumerate(row):
            wide = ref.shape[2]
            at = pl.ds(pl.multiple_of((me ^ mask) * wide, wide), wide) if len(row) * len(mixed) > 1 else slice(None)
            part = tokens[:, :, at].astype(F32).reshape(count * each, wide) + ref[j].astype(F32)
            resid[:, at] = part
            squares = part * part if squares is None else squares + part * part
    scale = lax.rsqrt(jnp.sum(squares, axis=-1, keepdims=True) / size + EPS)
    moe[...] = (resid[...] * scale * gain[...]).astype(BF16)
    own[...] = resid[pl.ds(pl.multiple_of(me * each, each), each), :]


def expert_kernel(rows_in, route, mix, d_gate, d_up, d_down, e_gate, e_up, e_down, out):
    x = rows_in[...]
    dot = functools.partial(jnp.dot, preferred_element_type=F32)
    hidden = (silu(dot(x, e_gate[...])) * dot(x, e_up[...])).astype(BF16)
    dense = (silu(dot(x, d_gate[...])) * dot(x, d_up[...])).astype(BF16)
    factor = jnp.sum(x.astype(F32) * mix[...].astype(F32), axis=1, keepdims=True)
    factor = 1.0 / (1.0 + jnp.exp(-factor))
    out[...] = (route[...] * dot(hidden, e_down[...]) + factor * dot(dense, d_down[...])).astype(out.dtype)


def fold_kernel(masks, where, own, other, *outs):
    me = where[0]
    each = outs[0].shape[1]
    for out, row in zip(outs, masks):
        for j, mask in enumerate(row):
            at = pl.ds(pl.multiple_of((me ^ mask) * each, each), each)
            out[j] = (own[at, :].astype(F32) + other[at, :].astype(F32)).astype(BF16)


def sum_kernel(parts, *refs):
    outs = refs[parts:]
    for i, out in enumerate(outs):
        total = refs[0][i].astype(F32)
        for ref in refs[1:parts]:
            total = total + ref[i].astype(F32)
        out[...] = total.astype(out.dtype)


def last_kernel(resid, *refs):
    total = refs[0][...].astype(F32)
    for ref in refs[1:-1]:
        total = total + ref[...].astype(F32)
    refs[-1][...] = (resid[...] + total).astype(refs[-1].dtype)


def body(
    tokens,
    mix_gain,
    w_query,
    w_key,
    w_value,
    w_zgate,
    w_beta,
    w_decay,
    decay_rate,
    decay_bias,
    head_gain,
    state,
    w_out,
    moe_gain,
    dense_mix,
    dense_gate,
    dense_up,
    dense_down,
    expert_gate,
    expert_up,
    expert_down,
    expert_ids,
    route_weight,
):
    ep_count = lax.axis_size("ep")
    me, par = lax.axis_index("ep"), lax.axis_index("tp")
    where = jnp.stack([me, par]).astype(jnp.int32)
    digits = digits_of(ep_count)
    masks = masks_of(digits)
    each, width = tokens.shape
    seqs, heads, size = state.shape[:3]
    half = ep_count * each
    sds = jax.ShapeDtypeStruct

    flat = [w.transpose(1, 2, 0).reshape(-1, width) for w in (w_query, w_key, w_value, w_zgate)]
    columns = 4 * flat[0].shape[0]
    early = seqs * 5 // 16
    parts = ((early, heads * size, size), (seqs - early, heads * size, size))
    by_rows = state.reshape(seqs, heads * size, size)
    near_tokens, near_first, short_first = call(
        bring_kernel,
        (sds(tokens.shape, BF16), sds(parts[0], F32), sds(parts[0], BF16)),
        [where, tokens, by_rows],
        smem=(),
        hbm=(1, 2),
        loose=(0,),
        scratch=[pltpu.SemaphoreType.DMA, pltpu.SemaphoreType.DMA((early,))],
    )
    tok_pieces = gather_xor(tokens, digits, near_tokens)
    stacked, gain_near, near, short = call(
        load_kernel,
        (
            sds((width, columns), BF16),
            sds((1, width), F32),
            sds(parts[1], F32),
            sds(parts[1], BF16),
        ),
        [tok_pieces[0], *flat, mix_gain[None], by_rows],
        scratch=[VM((columns, width), BF16), pltpu.SemaphoreType.DMA((5,)), pltpu.SemaphoreType.DMA((seqs - early,))],
        smem=(),
        hbm=range(1, 7),
        loose=(0,),
        spare=6,
    )
    normed = call(
        functools.partial(norm_kernel, masks),
        sds((ep_count, each, width), BF16),
        [where, *tok_pieces, gain_near, stacked],
        loose=(len(masks) + 2,),
    )
    normed_other = exchange(normed, 0, 1)
    order = digits[::-1]
    sent, came = scatter_masks(order)
    projected = call(project_own_kernel, sds((ep_count, each, columns), BF16), [normed, stacked], smem=(), spare=3)
    projected = call(
        functools.partial(project_kernel, sent),
        tuple(sds((len(row), 2, each, columns), BF16) for row in sent),
        [where, normed_other, projected, stacked],
        scratch=[VM((ep_count, each, columns), BF16)],
        spare=3,
    )
    by_seq = scatter_xor(projected, order)
    beta, retain, route, route_other, ordered = call(
        functools.partial(rates_kernel, masks),
        (
            sds((2, each, heads), F32),
            sds((2, each, heads), F32),
            sds((half, 1), F32),
            sds((half, 1), F32),
            sds((ep_count, each, width), BF16),
        ),
        [
            where,
            normed,
            normed_other,
            w_beta.T,
            w_decay.T,
            decay_rate[None],
            decay_bias[None],
            expert_ids.T,
            route_weight.T,
            *tok_pieces,
        ],
        scratch=[VM((ep_count, 2, each, 1), F32)],
    )
    gated, k_rows, keep, change = run_state(
        came,
        where,
        by_seq,
        beta.reshape(seqs, heads),
        retain.reshape(seqs, heads),
        head_gain[None],
        (short_first, short),
        state.shape,
    )

    gated_pieces = gather_xor(gated, digits)
    new_state = run_store(k_rows, keep, change, near_first, near, gated_pieces[0], state.shape)
    out_cols = w_out.shape[1]
    mixed, mixed_other = call(
        functools.partial(mix_kernel, masks),
        (sds((ep_count, each, out_cols), BF16), sds((ep_count, each, out_cols), BF16)),
        [where, *gated_pieces, w_out],
        scratch=[VM((2, ep_count, each, out_cols), BF16)],
    )
    mixed_other = exchange(mixed_other, 0, 1)
    mixed = call(pair_kernel, sds((half, out_cols), BF16), [mixed, mixed_other], smem=())
    mixed_pieces = gather_xor(mixed, digits)
    if out_cols % 128:
        order = jnp.argsort(me ^ jnp.array([m for row in masks for m in row], jnp.int32))
        blocks = jnp.take(jnp.concatenate(mixed_pieces, axis=0), order, axis=0)
        mixed_pieces = [blocks.transpose(1, 0, 2).reshape(1, half, width)]
    moe_in, resid = call(
        functools.partial(resid_kernel, masks if out_cols % 128 == 0 else [[0]]),
        (sds((half, width), BF16), sds((each, width), F32)),
        [where, ordered, *mixed_pieces, moe_gain[None]],
        scratch=[VM((half, width), F32)],
    )
    moe_other = exchange(moe_in, 0, 1)

    weights = [dense_mix[None], dense_gate, dense_up, dense_down, expert_gate[0], expert_up[0], expert_down[0]]
    run = lambda x, r, dt: call(expert_kernel, sds((half, width), dt), [x, r, *weights], smem=(), spare=6)
    part_own = run(moe_in, route, F32)
    part_other = run(moe_other, route_other, BF16)

    prev = len(masks[0])
    parts = call(
        functools.partial(fold_kernel, masks),
        tuple(sds((prev, each, width), BF16) for _ in masks),
        [where, part_own, exchange(part_other, 0, 1)],
    )
    for level in range(len(digits) - 1, 0, -1):
        shift, radix = digits[level]
        got = exchange_all(parts, shift, radix)
        nxt = digits[level - 1][1]
        got = [g.reshape(nxt, -1, width) for g in got]
        parts = call(
            functools.partial(sum_kernel, len(got)),
            tuple(sds(got[0].shape[1:], BF16) for _ in range(nxt)),
            got,
            smem=(),
        )
    shift, radix = digits[0]
    got = exchange_all(parts, shift, radix)
    layer_out = call(last_kernel, sds((each, width), BF16), [resid, *got], smem=())
    return (layer_out, new_state)


def solution(mesh):
    placed = (
        P(("ep", "tp"), None),
        P(),
        P(None, "tp", "ep"),
        P(None, "tp", "ep"),
        P(None, "tp", "ep"),
        P(None, "tp", "ep"),
        P(None, "tp"),
        P(None, "tp"),
        P("tp"),
        P("tp"),
        P(),
        P("ep", "tp", None, None),
        P("tp", "ep"),
        P(),
        P(),
        P(None, ("ep", "tp")),
        P(None, ("ep", "tp")),
        P(("ep", "tp"), None),
        P("ep", None, "tp"),
        P("ep", None, "tp"),
        P("ep", "tp", None),
        P(),
        P(),
    )
    return jax.shard_map(
        body,
        mesh=mesh,
        in_specs=placed,
        out_specs=(P(("ep", "tp"), None), P("ep", "tp", None, None)),
        check_vma=False,
    )
```
